32 devices in a mesh: rep: 2 (over x), fs: 4 (over y, core), tp: 4 (over z).
Axes of the slice: x: 2, y: 2, z: 4, core: 2. Of those that a mesh axis runs over, the one named last changes fastest.
Arguments:
- acts: bfloat16 [2048, 2048], P(('rep', 'fs'), 'tp'), may hold values from -6 to 6
- cotangent: bfloat16 [2048, 2048], P(('rep', 'fs'), 'tp'), may hold values from -8 to 8
- pre_act: bfloat16 [2048, 4096], P(('rep', 'fs'), 'tp'), may hold values from -6 to 6
- up_store: float32 [2048, 4096], P('fs', 'tp'), may hold values from -0.125 to 0.125
- up_scale: float32 [4096], P('tp'), may hold values from 0.5 to 2
- down_store: float32 [4096, 2048], P('tp', 'fs'), may hold values from -0.09375 to 0.09375
- down_scale: float32 [2048], replicated, may hold values from 0.5 to 2
Outputs:
- grad_input: bfloat16 [2048, 2048], P(('rep', 'fs'), 'tp')
- grad_up: float32 [2048, 4096], P('fs', 'tp')
- grad_down: float32 [4096, 2048], P('tp', 'fs')
The draws below stay inside these ranges and needn't reach their ends.
All inputs are finite; a program needn't handle non-finite values.
Results may differ from the reference program's by a relative error of at most 0.007.
Values may be sent and summed in bfloat16 or wider, within the bound.
A program may use at most 128 MiB of HBM per device.

```python
import math
import jax
import jax.numpy as jnp

D = 2048
FF = 4096
TOKENS = 2048


def with_spikes(entries, rng, source, target, blocks, factor):
    owner, partner = [(jnp.arange(entries.shape[dim]) // (entries.shape[dim] // blocks)).reshape([-1 if axis == dim else 1 for axis in range(entries.ndim)]) for dim in (source, target)]
    chosen = jax.random.permutation(rng, blocks)[partner]
    strong = (owner == chosen) | (owner == (partner + blocks // 2) % blocks)
    return jnp.where(strong, factor * entries, entries)


def block_scale(own_key, shape, split, smallest, high):
    gain, own = 1.0, jax.random.fold_in(own_key, 6)
    for axis_at, parts in split:
        draws = jnp.exp(jax.random.uniform(jax.random.fold_in(own, axis_at), (parts,), jnp.float32, smallest / len(split), high / len(split)))
        gain = gain * jnp.repeat(draws, shape[axis_at] // parts).reshape([-1 if axis == axis_at else 1 for axis in range(len(shape))])
    return gain


def noise(stream_key, shape, scale, limit, pieces=(), kind=jnp.bfloat16):
    result = jax.random.normal(stream_key, shape, jnp.float32) * scale
    if len(pieces) > 0:
        result = block_scale(stream_key, shape, pieces, -0.22, 0.18) * result
    return jnp.clip(result, min=-limit, max=limit).astype(kind)


def gaussian_with(key, dims, spread, bound, cuts, heavy, dtype=jnp.bfloat16):
    array = spread * jax.random.normal(key, dims, jnp.float32)
    if cuts:
        array = array * block_scale(key, dims, cuts, -0.22, 0.18)
    return jnp.clip(with_spikes(array, jax.random.fold_in(key, 3), *heavy), -bound, bound).astype(dtype)


def setup_inputs(seed: int = 0) -> dict:
    arg_keys = jax.random.split(jax.random.key(seed), 8)
    return {
        "acts": noise(arg_keys[0], (TOKENS, D), 1.0, 6.0, ((0, 8), (1, 4))),
        "cotangent": gaussian_with(arg_keys[1], (TOKENS, D), 1.0, 8.0, ((0, 8), (1, 4)), (0, 1, 8, 2.0)),
        "pre_act": noise(arg_keys[2], (TOKENS, FF), 1.0, 6.0, ((0, 8), (1, 4))),
        "up_store": noise(arg_keys[3], (D, FF), D ** -0.5, 0.125, ((0, 4), (1, 4)), jnp.float32),
        "up_scale": jnp.clip(jnp.exp(math.log(2.0) - 1.3862944 * jax.random.uniform(arg_keys[4], (FF,), jnp.float32) ** block_scale(arg_keys[4], (FF,), ((0, 4),), -0.2, 0.2)), 0.5, 2.0),
        "down_store": noise(arg_keys[5], (FF, D), FF ** -0.5, 0.09375, ((0, 4), (1, 4)), jnp.float32),
        "down_scale": jnp.clip(jnp.exp(jax.random.uniform(arg_keys[6], (D,), jnp.float32, math.log(0.5), math.log(2.0))), 0.5, 2.0),
    }


def reference(acts, cotangent, pre_act, up_store, up_scale, down_store, down_scale):
    norm_factor = 1.0 / math.sqrt(TOKENS)
    scaled = (cotangent.astype(jnp.float32) * down_scale[None, :]).astype(jnp.bfloat16)
    d_act = jnp.dot(scaled, down_store.astype(jnp.bfloat16).T, preferred_element_type=jnp.float32)
    positive = jnp.maximum(pre_act.astype(jnp.float32), 0.0)
    act = (positive * positive).astype(jnp.bfloat16)
    d_pre = (2.0 * positive * d_act * up_scale[None, :]).astype(jnp.bfloat16)
    grad_down = jnp.dot(act.T, scaled, preferred_element_type=jnp.float32) * norm_factor
    grad_up = jnp.dot(acts.T, d_pre, preferred_element_type=jnp.float32) * norm_factor
    grad_input = jnp.dot(d_pre, up_store.astype(jnp.bfloat16).T, preferred_element_type=jnp.float32).astype(jnp.bfloat16)
    return (grad_input, grad_up, grad_down)
```

```python
import functools
import math

import jax
import jax.numpy as jnp
from jax import lax
from jax.experimental import pallas as pl
from jax.experimental.pallas import tpu as pltpu
from jax.sharding import PartitionSpec as P

F32, BF16 = jnp.float32, jnp.bfloat16


def dot(left, right, dims):
    return lax.dot_general(left, right, (dims, ((), ())), preferred_element_type=F32)


def fitting(size, most):
    return most if size % most == 0 else size


def general_kernel(
    sizes,
    acts, cotangent, pre_act, up_store, up_scale, down_store, down_scale,
    grad_input, grad_up, grad_down,
    up_f32, down_f32,
    blocks, scaled_cols, acts_cols, act_group, dpre_group, down_bf, up_bf,
    pair_out, pair_in, far_out, far_in, d_act, gi_out, gi_mid, gi_in,
    gd_out, gd_in, gu_out, gu_in,
    load_sem,
    z_send, z_recv, col_send, col_recv, act_send, act_recv, dpre_send, dpre_recv,
    pair_send, pair_recv, far_send, far_recv, mid_send, mid_recv, gi_send, gi_recv,
    gd_send, gd_recv, gu_send, gu_recv,
):
    reps, F, T = sizes
    n, d = acts.shape
    h = pre_act.shape[1]
    w = down_store.shape[1]
    half, sub = F // 2, F // T
    chunks, cw = blocks.shape[2], blocks.shape[4]
    per = w // cw
    parts, hp = dpre_group.shape[0], dpre_group.shape[2]
    norm_factor = 1.0 / math.sqrt(n * F * reps)
    r, f, z = lax.axis_index("rep"), lax.axis_index("fs"), lax.axis_index("tp")
    core, place = lax.rem(f, 2), lax.div(f, 2)
    partner = f + 1 - 2 * core
    mesh_ids = pl.DeviceIdType.MESH

    down_load = pltpu.make_async_copy(down_store, down_f32, load_sem.at[0])
    up_load = pltpu.make_async_copy(up_store, up_f32, load_sem.at[1])
    down_load.start()
    up_load.start()

    barrier = pltpu.get_barrier_semaphore()

    def greet(at, carry):
        to_f, to_z = lax.div(at, T), lax.rem(at, T)

        @pl.when((to_f != f) | (to_z != z))
        def _():
            pl.semaphore_signal(
                barrier, inc=1, device_id={"fs": to_f, "tp": to_z}, device_id_type=mesh_ids
            )

        return carry

    lax.fori_loop(0, F * T, greet, 0)
    for p in range(1, reps):
        pl.semaphore_signal(
            barrier, inc=1, device_id={"rep": lax.rem(r + p, reps)}, device_id_type=mesh_ids
        )

    def rows(at):
        return pl.ds(pl.multiple_of(at * n, n), n)

    def remote(src, dst, send, recv, where):
        return pltpu.make_async_remote_copy(
            src_ref=src, dst_ref=dst, send_sem=send, recv_sem=recv,
            device_id=where, device_id_type=mesh_ids,
        )

    def landed(ref, recv):
        remote(ref, ref, recv, recv, {"fs": partner}).wait_recv()

    def left_for(ref, send):
        remote(ref, ref, send, send, {"fs": partner}).wait_send()

    cols = (scaled_cols, acts_cols)

    def pass_on(a, block, g, way):
        @pl.when((z < T - 1) if way == 0 else (z > 0))
        def _():
            ref = blocks.at[a, block, g]
            to = z + 1 if way == 0 else z - 1
            remote(ref, ref, z_send.at[a, block, g, way], z_recv.at[a, block, g], {"tp": to}).start()

    def spread(a, block, g):
        target, q = block * sub + g // per, g % per

        @pl.when(target != f)
        def _():
            remote(
                blocks.at[a, block, g], cols[a].at[q, rows(f)],
                col_send.at[a, block, g], col_recv.at[a, f, q], {"fs": target},
            ).start()

        @pl.when(target == f)
        def _():
            cols[a][q, rows(f), :] = blocks[a, block, g]

    def own_block(a):
        for g in range(chunks):
            pass_on(a, z, g, 0)
            pass_on(a, z, g, 1)
        for g in range(chunks):
            spread(a, z, g)

    def arriving(a, s):
        for g in range(chunks):
            @pl.when(z - s >= 0)
            def _():
                landed(blocks.at[a, z - s, g], z_recv.at[a, z - s, g])
                pass_on(a, z - s, g, 0)
                spread(a, z - s, g)

            @pl.when(z + s <= T - 1)
            def _():
                landed(blocks.at[a, z + s, g], z_recv.at[a, z + s, g])
                pass_on(a, z + s, g, 1)
                spread(a, z + s, g)

    def cols_landed(a, source):
        @pl.when(source != f)
        def _():
            for q in range(per):
                landed(cols[a].at[q, rows(source)], col_recv.at[a, source, q])

    def group_start(group, send, recv):
        ref = group.at[rows(f)]
        for k in range(1, half):
            to = lax.rem(f + 2 * k, F)
            remote(ref, ref, send.at[k], recv.at[f], {"fs": to}).start()
        remote(ref, ref, send.at[0], recv.at[f], {"fs": partner}).start()

    def group_forward(group, send, recv):
        for k in range(1, half):
            source = lax.rem(f - 2 * k + F, F)
            ref = group.at[rows(source)]
            landed(ref, recv.at[source])
            remote(ref, ref, send.at[half - 1 + k], recv.at[source], {"fs": partner}).start()

    def forwards_landed(group, recv):
        for k in range(1, half):
            source = lax.rem(partner + 2 * k, F)
            landed(group.at[rows(source)], recv.at[source])

    def group_sent(group, send):
        for k in range(F - 1):
            left_for(group.at[rows(f)], send.at[k])

    scale = down_scale[:, pl.ds(pl.multiple_of(z * d, d), d)]
    scaled = (cotangent[...].astype(F32) * scale).astype(BF16)
    for g in range(chunks):
        blocks[0, z, g] = scaled[:, g * cw:(g + 1) * cw]
    positive = jnp.maximum(pre_act[...].astype(F32), 0.0)
    act_group[rows(f), :] = (positive * positive).astype(BF16)
    pl.semaphore_wait(barrier, F * T - 1 + reps - 1)
    own_block(0)
    group_start(act_group, act_send, act_recv)
    for g in range(chunks):
        blocks[1, z, g] = acts[:, g * cw:(g + 1) * cw]
    down_load.wait()
    down_bf[...] = down_f32[...].astype(BF16)
    for s in range(1, T):
        if s == T - 1:
            group_forward(act_group, act_send, act_recv)
        arriving(0, s)
    own_block(1)

    def partial_of(target, e):
        value = jnp.zeros((n, hp), F32)
        for q in range(per):
            value = value + dot(
                scaled_cols[q, rows(target), :],
                down_bf[e * hp:(e + 1) * hp, q * cw:(q + 1) * cw], ((1,), (1,)),
            )
        return value

    for e in range(parts):
        def for_partner(k, carry):
            i = lax.rem(place + k, half)
            if e == 0:
                cols_landed(0, 2 * i + 1 - core)
            pair_out[e, i] = partial_of(2 * i + 1 - core, e).astype(BF16)
            remote(
                pair_out.at[e, i], pair_in.at[e, i], pair_send.at[e, i], pair_recv.at[e, i],
                {"fs": partner},
            ).start()
            return carry

        lax.fori_loop(1, half + 1, for_partner, 0)
    for e in range(parts):
        def for_far(k, carry):
            i = lax.rem(place + k, half)
            if e == 0:
                cols_landed(0, 2 * i + core)
            value = partial_of(2 * i + core, e)
            landed(pair_in.at[e, i], pair_recv.at[e, i])
            far_out[e, i] = (value + pair_in[e, i].astype(F32)).astype(BF16)
            remote(
                far_out.at[e, i], far_in.at[e, place], far_send.at[e, i], far_recv.at[e, place],
                {"fs": 2 * i + core},
            ).start()
            return carry

        lax.fori_loop(1, half, for_far, 0)
    for e in range(parts):
        value = partial_of(f, e)
        landed(pair_in.at[e, place], pair_recv.at[e, place])
        d_act[e] = value + pair_in[e, place].astype(F32)

    landed(act_group.at[rows(partner)], act_recv.at[partner])
    forwards_landed(act_group, act_recv)
    gd_rows = gd_out.shape[1]

    def rep_copy(out, into, send, recv, c, p):
        to = lax.rem(r + p, reps)
        return remote(
            out.at[c], into.at[p - 1, c], send.at[p - 1, c], recv.at[p - 1, c], {"rep": to}
        )

    def down_step(c, carry):
        at = pl.ds(pl.multiple_of(c * gd_rows, gd_rows), gd_rows)
        for q in range(per):
            value = dot(act_group[:, at], scaled_cols[q], ((0,), (0,))) * norm_factor
            gd_out[c, :, q * cw:(q + 1) * cw] = value.astype(BF16)
        for p in range(1, reps):
            rep_copy(gd_out, gd_in, gd_send, gd_recv, c, p).start()
        return carry

    lax.fori_loop(0, gd_out.shape[0], down_step, 0)
    arriving(1, 1)
    for e in range(parts):
        total = d_act[e]
        for k in range(1, half):
            j = lax.rem(place + k, half)
            landed(far_in.at[e, j], far_recv.at[e, j])
            total = total + far_in[e, j].astype(F32)
        at = slice(e * hp, (e + 1) * hp)
        positive = jnp.maximum(pre_act[:, at].astype(F32), 0.0)
        dpre_group[e, rows(f), :] = (2.0 * positive * total * up_scale[:, at]).astype(BF16)
        group_start(dpre_group.at[e], dpre_send.at[e], dpre_recv.at[e])
        if e == 0:
            up_load.wait()
            up_bf[...] = up_f32[...].astype(BF16)
            for s in range(2, T - 1):
                arriving(1, s)
    if T > 2:
        arriving(1, T - 1)

    def send_home(ref, source):
        home, slot = lax.div(source, sub), z * sub + lax.rem(source, sub)

        @pl.when(home != z)
        def _():
            remote(
                ref, gi_in.at[slot], gi_send.at[source], gi_recv.at[slot], {"tp": home}
            ).start()

        @pl.when(home == z)
        def _():
            gi_in[slot] = ref[...]

    def input_part(source):
        value = jnp.zeros((n, w), F32)
        for e in range(parts):
            value = value + dot(
                dpre_group[e, rows(source), :], up_bf[:, e * hp:(e + 1) * hp], ((1,), (1,))
            )
        gi_out[source] = value.astype(BF16)

        if source is f:
            send_home(gi_out.at[source], f)
        else:
            remote(
                gi_out.at[source], gi_mid.at[f], mid_send.at[source], mid_recv.at[f],
                {"fs": source},
            ).start()

    def relay(source):
        landed(gi_mid.at[source], mid_recv.at[source])
        send_home(gi_mid.at[source], source)

    input_part(f)
    for e in range(parts):
        landed(dpre_group.at[e, rows(partner)], dpre_recv.at[e, partner])
    input_part(partner)
    relay(partner)

    def up_step(e):
        forwards_landed(dpre_group.at[e], dpre_recv.at[e])
        for q in range(per):
            value = dot(acts_cols[q], dpre_group[e], ((0,), (0,)))
            gu_out[e, q * cw:(q + 1) * cw, :] = (value * norm_factor).astype(BF16)
        for p in range(1, reps):
            rep_copy(gu_out, gu_in, gu_send, gu_recv, e, p).start()

    for e in range(parts):
        group_forward(dpre_group.at[e], dpre_send.at[e], dpre_recv.at[e])
        if e == 0:
            for source in range(F):
                cols_landed(1, source)
        if e < parts - 1:
            up_step(e)
    for k in range(1, half):
        input_part(lax.rem(f + 2 * k, F))
    forwards_landed(dpre_group.at[parts - 1], dpre_recv.at[parts - 1])
    for k in range(1, half):
        input_part(lax.rem(partner + 2 * k, F))
    for q in range(per):
        value = dot(acts_cols[q], dpre_group[parts - 1], ((0,), (0,)))
        gu_out[parts - 1, q * cw:(q + 1) * cw, :] = (value * norm_factor).astype(BF16)
    for p in range(1, reps):
        rep_copy(gu_out, gu_in, gu_send, gu_recv, parts - 1, p).start()
    for k in range(1, half):
        relay(lax.rem(f + 2 * k, F))
        relay(lax.rem(partner + 2 * k, F))

    def total_of(out, into, send, recv, c):
        for p in range(1, reps):
            rep_copy(out, into, send, recv, c, p).wait()
        value = out[c].astype(F32)
        for p in range(1, reps):
            value = value + into[p - 1, c].astype(F32)
        return value

    def finish_down(c, carry):
        at = pl.ds(pl.multiple_of(c * gd_rows, gd_rows), gd_rows)
        grad_down[at, :] = total_of(gd_out, gd_in, gd_send, gd_recv, c)
        return carry

    lax.fori_loop(0, gd_out.shape[0], finish_down, 0)
    for e in range(parts - 1):
        grad_up[:, e * hp:(e + 1) * hp] = total_of(gu_out, gu_in, gu_send, gu_recv, e)
    for j in range(sub):
        value = jnp.zeros((n, w), F32)
        for s in range(T):
            at = s * sub + j

            @pl.when(s != z)
            def _():
                landed(gi_in.at[at], gi_recv.at[at])

            value = value + gi_in[at].astype(F32)
        grad_input[:, j * w:(j + 1) * w] = value.astype(BF16)
    grad_up[:, (parts - 1) * hp:] = total_of(gu_out, gu_in, gu_send, gu_recv, parts - 1)

    for a in range(2):
        for block in range(T):
            for g in range(chunks):
                @pl.when((block <= z) & (z < T - 1))
                def _():
                    left_for(blocks.at[a, block, g], z_send.at[a, block, g, 0])

                @pl.when((block >= z) & (z > 0))
                def _():
                    left_for(blocks.at[a, block, g], z_send.at[a, block, g, 1])

                @pl.when(block * sub + g // per != f)
                def _():
                    left_for(blocks.at[a, block, g], col_send.at[a, block, g])
    group_sent(act_group, act_send)
    for e in range(parts):
        group_sent(dpre_group.at[e], dpre_send.at[e])
        for i in range(half):
            left_for(pair_out.at[e, i], pair_send.at[e, i])

            @pl.when(i != place)
            def _():
                left_for(far_out.at[e, i], far_send.at[e, i])
    for source in range(F):
        @pl.when(source != f)
        def _():
            left_for(gi_out.at[source], mid_send.at[source])

        @pl.when(source // sub != z)
        def _():
            left_for(gi_mid.at[source], gi_send.at[source])


def general_body(sizes, acts, cotangent, pre_act, up_store, up_scale, down_store, down_scale):
    reps, F, T = sizes
    n, d = acts.shape
    h = pre_act.shape[1]
    w = down_store.shape[1]
    half = F // 2
    cw = w // 2 if w % 256 == 0 else w
    per, chunks = w // cw, d // cw
    parts = 2 if h % 256 == 0 else 1
    hp = h // parts
    gd_rows = fitting(h, 256)
    gd_steps = h // gd_rows
    others = max(reps - 1, 1)
    sem = pltpu.SemaphoreType.DMA
    vmem, anywhere = (pl.BlockSpec(memory_space=s) for s in (pltpu.VMEM, pltpu.HBM))
    arrays = [
        ((w, h), F32), ((h, w), F32),
        ((2, T, chunks, n, cw), BF16),
        ((per, F * n, cw), BF16), ((per, F * n, cw), BF16),
        ((F * n, h), BF16), ((parts, F * n, hp), BF16),
        ((h, w), BF16), ((w, h), BF16),
        ((parts, half, n, hp), BF16), ((parts, half, n, hp), BF16),
        ((parts, half, n, hp), BF16), ((parts, half, n, hp), BF16),
        ((parts, n, hp), F32),
        ((F, n, w), BF16), ((F, n, w), BF16), ((F, n, w), BF16),
        ((gd_steps, gd_rows, w), BF16), ((others, gd_steps, gd_rows, w), BF16),
        ((parts, w, hp), BF16), ((others, parts, w, hp), BF16),
    ]
    return pl.pallas_call(
        functools.partial(general_kernel, sizes),
        out_shape=(
            jax.ShapeDtypeStruct((n, d), BF16),
            jax.ShapeDtypeStruct((w, h), F32),
            jax.ShapeDtypeStruct((h, w), F32),
        ),
        in_specs=[vmem, vmem, vmem, anywhere, vmem, anywhere, vmem],
        out_specs=(vmem, vmem, vmem),
        scratch_shapes=[pltpu.VMEM(shape, kind) for shape, kind in arrays] + [
            sem((2,)),
            sem((2, T, chunks, 2)), sem((2, T, chunks)), sem((2, T, chunks)), sem((2, F, per)),
            sem((F,)), sem((F,)), sem((parts, F)), sem((parts, F)),
            sem((parts, half)), sem((parts, half)), sem((parts, half)), sem((parts, half)),
            sem((F,)), sem((F,)), sem((F,)), sem((F,)),
            sem((others, gd_steps)), sem((others, gd_steps)),
            sem((others, parts)), sem((others, parts)),
        ],
        compiler_params=pltpu.CompilerParams(
            collective_id=0, has_side_effects=True,
            vmem_limit_bytes=60 * 1024 * 1024,
        ),
    )(
        acts, cotangent, pre_act, up_store, up_scale.reshape(1, h), down_store,
        down_scale.reshape(1, d * T),
    )


def square_kernel(
    sizes,
    acts, cotangent, pre_act, up_store, up_scale, down_store, down_scale,
    gd_out, gd_in, gu_out, gu_in, gi_in,
    acts_v, cot_v, pre_v, up_f32, up_scale_v, down_f32, down_scale_v,
    own, scaled_cols, acts_cols, act_group, dpre_group, down_bf, up_bf,
    pair_out, pair_in, far_out, far_in, d_act, gi_out, gi_mid,
    load_sem,
    org_send, fwd_send, col_recv, act_send, act_recv, dpre_send, dpre_recv,
    pair_send, pair_recv, far_send, far_recv,
    mid_send, mid_recv, gi_send, gi_recv, relay_send,
    gd_send, gd_recv, gu_send, gu_recv,
):
    reps, F, T = sizes
    n, d = acts.shape
    h = pre_act.shape[1]
    w = down_store.shape[1]
    parts, hp = dpre_group.shape[0], dpre_group.shape[2]
    steps, gd_rows = gd_out.shape[0], gd_out.shape[1]
    tiles, gu_rows = gu_out.shape[1], gu_out.shape[2]
    pieces = col_recv.shape[2]
    rp = n // pieces
    norm_factor = 1.0 / math.sqrt(n * F * reps)
    r, f, z = lax.axis_index("rep"), lax.axis_index("fs"), lax.axis_index("tp")
    core, place = lax.rem(f, 2), lax.div(f, 2)
    partner = f + 1 - 2 * core
    across = lax.rem(f + 2, F)
    corner = lax.rem(partner + 2, F)
    z_pair, z_far = z + 1 - 2 * lax.rem(z, 2), lax.rem(z + 2, T)
    mesh_ids = pl.DeviceIdType.MESH

    loads = [
        pltpu.make_async_copy(src, dst, load_sem.at[i])
        for i, (src, dst) in enumerate((
            (cotangent, cot_v), (down_scale, down_scale_v), (pre_act, pre_v),
            (down_store, down_f32), (acts, acts_v), (up_scale, up_scale_v), (up_store, up_f32),
        ))
    ]
    for load in loads:
        load.start()

    barrier = pltpu.get_barrier_semaphore()

    def greet(at, carry):
        to_f, to_z = lax.div(at, T), lax.rem(at, T)

        @pl.when((to_f != f) | (to_z != z))
        def _():
            pl.semaphore_signal(
                barrier, inc=1, device_id={"fs": to_f, "tp": to_z}, device_id_type=mesh_ids
            )

        return carry

    lax.fori_loop(0, F * T, greet, 0)
    for p in range(1, reps):
        pl.semaphore_signal(
            barrier, inc=1, device_id={"rep": lax.rem(r + p, reps)}, device_id_type=mesh_ids
        )

    def rows(at):
        return pl.ds(pl.multiple_of(at * n, n), n)

    def piece(at, p):
        return pl.ds(pl.multiple_of(at * n + p * rp, rp), rp)

    def remote(src, dst, send, recv, where):
        return pltpu.make_async_remote_copy(
            src_ref=src, dst_ref=dst, send_sem=send, recv_sem=recv,
            device_id=where, device_id_type=mesh_ids,
        )

    def landed(ref, recv):
        remote(ref, ref, recv, recv, {"fs": partner}).wait_recv()

    def left_for(ref, send):
        remote(ref, ref, send, send, {"fs": partner}).wait_send()

    cols = (scaled_cols, acts_cols)
    sources = (own, acts_v)
    same = lax.div(z, 2) == place
    direct = (z == f) | (z_far == f)
    rises = (z > f) & (z < T - 1)
    falls = (z < f) & (z > 0)

    def originate(a, k, p, where):
        at = pl.ds(p * rp, rp)
        remote(
            sources[a].at[at], cols[a].at[piece(f, p)],
            org_send.at[a, k, p], col_recv.at[a, f, p], where,
        ).start()

    def originate_line(a):
        @pl.when(same)
        def _():
            for p in range(pieces):
                @pl.when(z < T - 1)
                def _():
                    originate(a, 1, p, {"fs": z, "tp": z + 1})

                @pl.when(z > 0)
                def _():
                    originate(a, 2, p, {"fs": z, "tp": z - 1})

                @pl.when(z != f)
                def _():
                    originate(a, 0, p, {"fs": z})

            @pl.when(z == f)
            def _():
                cols[a][rows(f), :] = sources[a][...]

    def originate_cross(a):
        @pl.when(jnp.logical_not(same))
        def _():
            for p in range(pieces):
                originate(a, 1, p, {"fs": z, "tp": z_far})
                originate(a, 0, p, {"fs": z})

    def pass_on(a, source, p, to):
        ref = cols[a].at[piece(source, p)]
        landed(ref, col_recv.at[a, source, p])
        remote(ref, ref, fwd_send.at[a, source, p], col_recv.at[a, source, p], {"tp": to}).start()

    def cross_forward(a):
        @pl.when(direct)
        def _():
            for p in range(pieces):
                for source in (across, corner):
                    pass_on(a, source, p, z_pair)

    def line_forward(a):
        @pl.when(rises)
        def _():
            for p in range(pieces):
                for source in (f, partner):
                    pass_on(a, source, p, z + 1)

        @pl.when(falls)
        def _():
            for p in range(pieces):
                for source in (f, partner):
                    pass_on(a, source, p, z - 1)

    def cross_rest(a):
        @pl.when(jnp.logical_not(direct))
        def _():
            for p in range(pieces):
                for source in (across, corner):
                    landed(cols[a].at[piece(source, p)], col_recv.at[a, source, p])

    def line_rest(a):
        for p in range(pieces):
            @pl.when(jnp.logical_not(rises | falls) & (z != f))
            def _():
                landed(cols[a].at[piece(f, p)], col_recv.at[a, f, p])

            @pl.when(jnp.logical_not(rises | falls))
            def _():
                landed(cols[a].at[piece(partner, p)], col_recv.at[a, partner, p])

    def act_across(p):
        ref = act_group.at[piece(f, p)]
        remote(ref, ref, act_send.at[0, p], act_recv.at[f, p], {"fs": across}).start()

    loads[0].wait()
    loads[1].wait()
    scale = down_scale_v[:, pl.ds(pl.multiple_of(z * d, d), d)]
    own[...] = (cot_v[...].astype(F32) * scale).astype(BF16)
    loads[2].wait()
    positive = jnp.maximum(pre_v[...].astype(F32), 0.0)
    act_group[rows(f), :] = (positive * positive).astype(BF16)
    loads[4].wait()
    pl.semaphore_wait(barrier, F * T - 1 + reps - 1)

    originate_cross(0)
    originate_line(0)
    for p in range(pieces - 1):
        act_across(p)
    for p in range(pieces):
        ref = act_group.at[piece(f, p)]
        remote(ref, ref, act_send.at[1, p], act_recv.at[f, p], {"fs": partner}).start()
    loads[3].wait()
    down_bf[...] = down_f32[...].astype(BF16)
    cross_forward(0)
    act_across(pieces - 1)
    line_forward(0)
    cross_rest(0)

    def partial_of(target, e):
        return dot(
            scaled_cols[rows(target), :], down_bf[e * hp:(e + 1) * hp, :], ((1,), (1,))
        )

    def to_partner(target, k, e):
        pair_out[k, e] = partial_of(target, e).astype(BF16)
        remote(
            pair_out.at[k, e], pair_in.at[k, e], pair_send.at[k, e], pair_recv.at[k, e],
            {"fs": partner},
        ).start()

    for e in range(parts):
        to_partner(corner, 0, e)
    for e in range(parts):
        value = partial_of(across, e)
        landed(pair_in.at[0, e], pair_recv.at[0, e])
        far_out[e] = (value + pair_in[0, e].astype(F32)).astype(BF16)
        remote(
            far_out.at[e], far_in.at[e], far_send.at[e], far_recv.at[e], {"fs": across}
        ).start()

    originate_line(1)
    originate_cross(1)
    for p in range(pieces):
        ref = act_group.at[piece(across, p)]
        landed(ref, act_recv.at[across, p])
        remote(ref, ref, act_send.at[2, p], act_recv.at[across, p], {"fs": partner}).start()
    line_rest(0)
    for e in range(parts):
        to_partner(partner, 1, e)
    for p in range(pieces):
        for source in (partner, corner):
            landed(act_group.at[piece(source, p)], act_recv.at[source, p])

    def rep_copy(out, into, send, recv, at, p):
        to = lax.rem(r + p, reps)
        return remote(
            out.at[at], into.at[(p - 1,) + at], send.at[(p - 1,) + at], recv.at[(p - 1,) + at],
            {"rep": to},
        )

    def down_step(c, carry):
        at = pl.ds(pl.multiple_of(c * gd_rows, gd_rows), gd_rows)
        value = dot(act_group[:, at], scaled_cols[...], ((0,), (0,))) * norm_factor
        gd_out[c] = value.astype(BF16)
        for p in range(1, reps):
            rep_copy(gd_out, gd_in, gd_send, gd_recv, (c,), p).start()
        return carry

    lax.fori_loop(0, steps, down_step, 0)
    for e in range(parts):
        value = partial_of(f, e)
        landed(pair_in.at[1, e], pair_recv.at[1, e])
        d_act[e] = value + pair_in[1, e].astype(F32)
    loads[5].wait()
    loads[6].wait()
    up_bf[...] = up_f32[...].astype(BF16)
    line_forward(1)

    for e in range(parts):
        landed(far_in.at[e], far_recv.at[e])
        total = d_act[e] + far_in[e].astype(F32)
        at = slice(e * hp, (e + 1) * hp)
        positive = jnp.maximum(pre_v[:, at].astype(F32), 0.0)
        dpre_group[e, rows(f), :] = (2.0 * positive * total * up_scale_v[:, at]).astype(BF16)
        ref = dpre_group.at[e, rows(f)]
        remote(ref, ref, dpre_send.at[0, e], dpre_recv.at[e, f], {"fs": across}).start()
        remote(ref, ref, dpre_send.at[1, e], dpre_recv.at[e, f], {"fs": partner}).start()

    cross_forward(1)

    def input_part(target, k):
        value = jnp.zeros((n, w), F32)
        for e in range(parts):
            value = value + dot(
                dpre_group[e, rows(target), :], up_bf[:, e * hp:(e + 1) * hp], ((1,), (1,))
            )
        gi_out[k] = value.astype(BF16)

    def half_rows(p):
        return pl.ds(p * rp, rp)

    input_part(f, 0)
    for p in range(pieces):
        @pl.when(z != f)
        def _():
            remote(
                gi_out.at[0, half_rows(p)], gi_in.at[z, half_rows(p)],
                gi_send.at[0, p], gi_recv.at[z, p], {"tp": f},
            ).start()

    @pl.when(z == f)
    def _():
        gi_in[z] = gi_out[0]

    for e in range(parts):
        landed(dpre_group.at[e, rows(partner)], dpre_recv.at[e, partner])
    input_part(partner, 1)
    for p in range(pieces):
        remote(
            gi_out.at[1, half_rows(p)], gi_in.at[z, half_rows(p)],
            gi_send.at[1, p], gi_recv.at[z, p], {"fs": partner, "tp": f},
        ).start()

    def up_step(e):
        landed(dpre_group.at[e, rows(corner)], dpre_recv.at[e, corner])
        for q in range(tiles):
            value = dot(
                acts_cols[:, q * gu_rows:(q + 1) * gu_rows], dpre_group[e], ((0,), (0,))
            )
            gu_out[e, q] = (value * norm_factor).astype(BF16)
            for p in range(1, reps):
                rep_copy(gu_out, gu_in, gu_send, gu_recv, (e, q), p).start()

    def cross_part(target, k):
        input_part(target, k)
        for p in range(pieces):
            @pl.when(z == f)
            def _():
                remote(
                    gi_out.at[k, half_rows(p)], gi_in.at[z, half_rows(p)],
                    gi_send.at[k, p], gi_recv.at[z, p], {"fs": target},
                ).start()

            @pl.when(z != f)
            def _():
                remote(
                    gi_out.at[k, half_rows(p)], gi_mid.at[core, half_rows(p)],
                    gi_send.at[k, p], mid_recv.at[core, p], {"fs": target},
                ).start()

    for e in range(parts):
        ref = dpre_group.at[e, rows(across)]
        landed(ref, dpre_recv.at[e, across])
        remote(ref, ref, dpre_send.at[2, e], dpre_recv.at[e, across], {"fs": partner}).start()
        if e == 0:
            cross_rest(1)
            line_rest(1)
        if e < parts - 1:
            up_step(e)
    cross_part(across, 2)
    landed(dpre_group.at[parts - 1, rows(corner)], dpre_recv.at[parts - 1, corner])
    cross_part(corner, 3)
    for q in range(tiles):
        value = dot(
            acts_cols[:, q * gu_rows:(q + 1) * gu_rows], dpre_group[parts - 1], ((0,), (0,))
        )
        gu_out[parts - 1, q] = (value * norm_factor).astype(BF16)
        for p in range(1, reps):
            rep_copy(gu_out, gu_in, gu_send, gu_recv, (parts - 1, q), p).start()

    for k in range(2):
        source = core if k == 0 else 1 - core
        home = 2 * (1 - place) + source

        @pl.when(z != home)
        def _():
            for p in range(pieces):
                ref = gi_mid.at[source, half_rows(p)]
                landed(ref, mid_recv.at[source, p])
                remote(
                    ref, gi_in.at[z, half_rows(p)], relay_send.at[k, p], gi_recv.at[z, p],
                    {"tp": home},
                ).start()

    for p in range(1, reps):
        for c in range(steps):
            rep_copy(gd_out, gd_in, gd_send, gd_recv, (c,), p).wait()
    for s in range(T):
        @pl.when((s != z) | (z != f))
        def _():
            for p in range(pieces):
                landed(gi_in.at[s, half_rows(p)], gi_recv.at[s, p])

    for p in range(pieces):
        for a in range(2):
            @pl.when(same & (z != f) | jnp.logical_not(same))
            def _():
                left_for(own.at[half_rows(p)], org_send.at[a, 0, p])

            @pl.when(same & (z < T - 1) | jnp.logical_not(same))
            def _():
                left_for(own.at[half_rows(p)], org_send.at[a, 1, p])

            @pl.when(same & (z > 0))
            def _():
                left_for(own.at[half_rows(p)], org_send.at[a, 2, p])

            @pl.when(direct)
            def _():
                for source in (across, corner):
                    left_for(own.at[half_rows(p)], fwd_send.at[a, source, p])

            @pl.when(rises | falls)
            def _():
                for source in (f, partner):
                    left_for(own.at[half_rows(p)], fwd_send.at[a, source, p])
        for k in range(3):
            left_for(act_group.at[piece(f, p)], act_send.at[k, p])

        @pl.when(z != f)
        def _():
            left_for(own.at[half_rows(p)], gi_send.at[0, p])

        for k in range(1, 4):
            left_for(own.at[half_rows(p)], gi_send.at[k, p])
        for k in range(2):
            source = core if k == 0 else 1 - core

            @pl.when(z != 2 * (1 - place) + source)
            def _():
                left_for(own.at[half_rows(p)], relay_send.at[k, p])
    for e in range(parts):
        for k in range(3):
            left_for(dpre_group.at[e, rows(f)], dpre_send.at[k, e])
        for k in range(2):
            left_for(pair_out.at[k, e], pair_send.at[k, e])
        left_for(far_out.at[e], far_send.at[e])
    for p in range(1, reps):
        for e in range(parts):
            for q in range(tiles):
                rep_copy(gu_out, gu_in, gu_send, gu_recv, (e, q), p).wait()


def finish_kernel(
    gd_out, gd_in, gu_out, gu_in, gi_in, grad_input, grad_up, grad_down,
    gi_v, gu_v, gd_v, gi_sem, gu_sem, gd_sem,
):
    others = gd_in.shape[0]
    steps, gd_rows = gd_out.shape[0], gd_out.shape[1]
    parts, tiles, gu_rows, hp = gu_out.shape
    copies = []

    def leave(src, dst, sem):
        copies.append(pltpu.make_async_copy(src, dst, sem))
        copies[-1].start()

    for c in range(steps):
        value = gd_out[c].astype(F32)
        for p in range(others):
            value = value + gd_in[p, c].astype(F32)
        gd_v[c] = value
        leave(gd_v.at[c], grad_down.at[pl.ds(c * gd_rows, gd_rows)], gd_sem.at[c])
    for e in range(parts):
        for q in range(tiles):
            value = gu_out[e, q].astype(F32)
            for p in range(others):
                value = value + gu_in[p, e, q].astype(F32)
            gu_v[e, q] = value
            at = (pl.ds(q * gu_rows, gu_rows), pl.ds(e * hp, hp))
            leave(gu_v.at[e, q], grad_up.at[at], gu_sem.at[e, q])
    value = gi_in[0].astype(F32)
    for s in range(1, gi_in.shape[0]):
        value = value + gi_in[s].astype(F32)
    gi_v[...] = value.astype(BF16)
    leave(gi_v, grad_input, gi_sem.at[0])
    for copy in copies:
        copy.wait()


def square_body(sizes, acts, cotangent, pre_act, up_store, up_scale, down_store, down_scale):
    reps, F, T = sizes
    n, d = acts.shape
    h = pre_act.shape[1]
    w = down_store.shape[1]
    parts = 2 if h % 256 == 0 else 1
    pieces = 2 if n % 32 == 0 else 1
    tiles = 2 if w % 256 == 0 else 1
    hp = h // parts
    gd_rows = fitting(h, 256)
    steps = h // gd_rows
    others = reps - 1
    sem = pltpu.SemaphoreType.DMA
    vmem, hbm = (pl.BlockSpec(memory_space=s) for s in (pltpu.VMEM, pltpu.HBM))
    shared = [
        (steps, gd_rows, w), (others, steps, gd_rows, w),
        (parts, tiles, w // tiles, hp), (others, parts, tiles, w // tiles, hp),
        (T, n, w),
    ]
    arrays = [
        ((n, d), BF16), ((n, d), BF16), ((n, h), BF16),
        ((w, h), F32), ((1, h), F32), ((h, w), F32), ((1, d * T), F32),
        ((n, d), BF16), ((F * n, w), BF16), ((F * n, w), BF16),
        ((F * n, h), BF16), ((parts, F * n, hp), BF16),
        ((h, w), BF16), ((w, h), BF16),
        ((2, parts, n, hp), BF16), ((2, parts, n, hp), BF16),
        ((parts, n, hp), BF16), ((parts, n, hp), BF16),
        ((parts, n, hp), F32),
        ((F, n, w), BF16), ((2, n, w), BF16),
    ]
    moved = pl.pallas_call(
        functools.partial(square_kernel, sizes),
        out_shape=tuple(jax.ShapeDtypeStruct(shape, BF16) for shape in shared),
        in_specs=[hbm] * 7,
        out_specs=(vmem,) * len(shared),
        scratch_shapes=[pltpu.VMEM(shape, kind) for shape, kind in arrays] + [
            sem((7,)),
            sem((2, 3, pieces)), sem((2, F, pieces)), sem((2, F, pieces)),
            sem((3, pieces)), sem((F, pieces)), sem((3, parts)), sem((parts, F)),
            sem((2, parts)), sem((2, parts)), sem((parts,)), sem((parts,)),
            sem((1,)), sem((2, pieces)), sem((4, pieces)), sem((T, pieces)), sem((2, pieces)),
            sem((others, steps)), sem((others, steps)),
            sem((others, parts, tiles)), sem((others, parts, tiles)),
        ],
        compiler_params=pltpu.CompilerParams(
            collective_id=0, has_side_effects=True,
            vmem_limit_bytes=40 * 1024 * 1024,
        ),
    )(*(
        pltpu.with_memory_space_constraint(array, pltpu.HBM)
        for array in (
            acts, cotangent, pre_act, up_store, up_scale.reshape(1, h), down_store,
            down_scale.reshape(1, d * T),
        )
    ))
    return pl.pallas_call(
        finish_kernel,
        out_shape=(
            jax.ShapeDtypeStruct((n, d), BF16),
            jax.ShapeDtypeStruct((w, h), F32),
            jax.ShapeDtypeStruct((h, w), F32),
        ),
        in_specs=[vmem] * len(shared),
        out_specs=(hbm,) * 3,
        scratch_shapes=[
            pltpu.VMEM((n, d), BF16),
            pltpu.VMEM((parts, tiles, w // tiles, hp), F32),
            pltpu.VMEM((steps, gd_rows, w), F32),
            sem((1,)), sem((parts, tiles)), sem((steps,)),
        ],
        compiler_params=pltpu.CompilerParams(vmem_limit_bytes=12 * 1024 * 1024),
    )(*moved)


def body(sizes, *arrays):
    reps, F, T = sizes
    square = F == T and F == 2 * 2 and reps > 1
    return (square_body if square else general_body)(sizes, *arrays)


def solution(mesh):
    sizes = (mesh.shape["rep"], mesh.shape["fs"], mesh.shape["tp"])
    return jax.shard_map(
        functools.partial(body, sizes),
        mesh=mesh,
        in_specs=(
            P(("rep", "fs"), "tp"),
            P(("rep", "fs"), "tp"),
            P(("rep", "fs"), "tp"),
            P("fs", "tp"),
            P("tp"),
            P("tp", "fs"),
            P(),
        ),
        out_specs=(P(("rep", "fs"), "tp"), P("fs", "tp"), P("tp", "fs")),
        check_vma=False,
    )
```

```python
import functools
import math

import jax
import jax.numpy as jnp
from jax import lax
from jax.experimental import pallas as pl
from jax.experimental.pallas import tpu as pltpu
from jax.sharding import PartitionSpec as P

F32, BF16 = jnp.float32, jnp.bfloat16


def dot(left, right, dims):
    return lax.dot_general(left, right, (dims, ((), ())), preferred_element_type=F32)


def fitting(size, most):
    return most if size % most == 0 else size


def general_kernel(
    sizes,
    acts, cotangent, pre_act, up_store, up_scale, down_store, down_scale,
    grad_input, grad_up, grad_down,
    up_f32, down_f32,
    blocks, scaled_cols, acts_cols, act_group, dpre_group, down_bf, up_bf,
    pair_out, pair_in, far_out, far_in, d_act, gi_out, gi_mid, gi_in,
    gd_out, gd_in, gu_out, gu_in,
    load_sem,
    z_send, z_recv, col_send, col_recv, act_send, act_recv, dpre_send, dpre_recv,
    pair_send, pair_recv, far_send, far_recv, mid_send, mid_recv, gi_send, gi_recv,
    gd_send, gd_recv, gu_send, gu_recv,
):
    reps, F, T = sizes
    n, d = acts.shape
    h = pre_act.shape[1]
    w = down_store.shape[1]
    half, sub = F // 2, F // T
    chunks, cw = blocks.shape[2], blocks.shape[4]
    per = w // cw
    parts, hp = dpre_group.shape[0], dpre_group.shape[2]
    norm_factor = 1.0 / math.sqrt(n * F * reps)
    r, f, z = lax.axis_index("rep"), lax.axis_index("fs"), lax.axis_index("tp")
    core, place = lax.rem(f, 2), lax.div(f, 2)
    partner = f + 1 - 2 * core
    mesh_ids = pl.DeviceIdType.MESH

    down_load = pltpu.make_async_copy(down_store, down_f32, load_sem.at[0])
    up_load = pltpu.make_async_copy(up_store, up_f32, load_sem.at[1])
    down_load.start()
    up_load.start()

    barrier = pltpu.get_barrier_semaphore()

    def greet(at, carry):
        to_f, to_z = lax.div(at, T), lax.rem(at, T)

        @pl.when((to_f != f) | (to_z != z))
        def _():
            pl.semaphore_signal(
                barrier, inc=1, device_id={"fs": to_f, "tp": to_z}, device_id_type=mesh_ids
            )

        return carry

    lax.fori_loop(0, F * T, greet, 0)
    for p in range(1, reps):
        pl.semaphore_signal(
            barrier, inc=1, device_id={"rep": lax.rem(r + p, reps)}, device_id_type=mesh_ids
        )

    def rows(at):
        return pl.ds(pl.multiple_of(at * n, n), n)

    def remote(src, dst, send, recv, where):
        return pltpu.make_async_remote_copy(
            src_ref=src, dst_ref=dst, send_sem=send, recv_sem=recv,
            device_id=where, device_id_type=mesh_ids,
        )

    def landed(ref, recv):
        remote(ref, ref, recv, recv, {"fs": partner}).wait_recv()

    def left_for(ref, send):
        remote(ref, ref, send, send, {"fs": partner}).wait_send()

    cols = (scaled_cols, acts_cols)

    def pass_on(a, block, g, way):
        @pl.when((z < T - 1) if way == 0 else (z > 0))
        def _():
            ref = blocks.at[a, block, g]
            to = z + 1 if way == 0 else z - 1
            remote(ref, ref, z_send.at[a, block, g, way], z_recv.at[a, block, g], {"tp": to}).start()

    def spread(a, block, g):
        target, q = block * sub + g // per, g % per

        @pl.when(target != f)
        def _():
            remote(
                blocks.at[a, block, g], cols[a].at[q, rows(f)],
                col_send.at[a, block, g], col_recv.at[a, f, q], {"fs": target},
            ).start()

        @pl.when(target == f)
        def _():
            cols[a][q, rows(f), :] = blocks[a, block, g]

    def own_block(a):
        for g in range(chunks):
            pass_on(a, z, g, 0)
            pass_on(a, z, g, 1)
        for g in range(chunks):
            spread(a, z, g)

    def arriving(a, s):
        for g in range(chunks):
            @pl.when(z - s >= 0)
            def _():
                landed(blocks.at[a, z - s, g], z_recv.at[a, z - s, g])
                pass_on(a, z - s, g, 0)
                spread(a, z - s, g)

            @pl.when(z + s <= T - 1)
            def _():
                landed(blocks.at[a, z + s, g], z_recv.at[a, z + s, g])
                pass_on(a, z + s, g, 1)
                spread(a, z + s, g)

    def cols_landed(a, source):
        @pl.when(source != f)
        def _():
            for q in range(per):
                landed(cols[a].at[q, rows(source)], col_recv.at[a, source, q])

    def group_start(group, send, recv):
        ref = group.at[rows(f)]
        for k in range(1, half):
            to = lax.rem(f + 2 * k, F)
            remote(ref, ref, send.at[k], recv.at[f], {"fs": to}).start()
        remote(ref, ref, send.at[0], recv.at[f], {"fs": partner}).start()

    def group_forward(group, send, recv):
        for k in range(1, half):
            source = lax.rem(f - 2 * k + F, F)
            ref = group.at[rows(source)]
            landed(ref, recv.at[source])
            remote(ref, ref, send.at[half - 1 + k], recv.at[source], {"fs": partner}).start()

    def forwards_landed(group, recv):
        for k in range(1, half):
            source = lax.rem(partner + 2 * k, F)
            landed(group.at[rows(source)], recv.at[source])

    def group_sent(group, send):
        for k in range(F - 1):
            left_for(group.at[rows(f)], send.at[k])

    scale = down_scale[:, pl.ds(pl.multiple_of(z * d, d), d)]
    scaled = (cotangent[...].astype(F32) * scale).astype(BF16)
    for g in range(chunks):
        blocks[0, z, g] = scaled[:, g * cw:(g + 1) * cw]
    positive = jnp.maximum(pre_act[...].astype(F32), 0.0)
    act_group[rows(f), :] = (positive * positive).astype(BF16)
    pl.semaphore_wait(barrier, F * T - 1 + reps - 1)
    own_block(0)
    group_start(act_group, act_send, act_recv)
    for g in range(chunks):
        blocks[1, z, g] = acts[:, g * cw:(g + 1) * cw]
    down_load.wait()
    down_bf[...] = down_f32[...].astype(BF16)
    for s in range(1, T):
        if s == T - 1:
            group_forward(act_group, act_send, act_recv)
        arriving(0, s)
    own_block(1)

    def partial_of(target, e):
        value = jnp.zeros((n, hp), F32)
        for q in range(per):
            value = value + dot(
                scaled_cols[q, rows(target), :],
                down_bf[e * hp:(e + 1) * hp, q * cw:(q + 1) * cw], ((1,), (1,)),
            )
        return value

    for e in range(parts):
        def for_partner(k, carry):
            i = lax.rem(place + k, half)
            if e == 0:
                cols_landed(0, 2 * i + 1 - core)
            pair_out[e, i] = partial_of(2 * i + 1 - core, e).astype(BF16)
            remote(
                pair_out.at[e, i], pair_in.at[e, i], pair_send.at[e, i], pair_recv.at[e, i],
                {"fs": partner},
            ).start()
            return carry

        lax.fori_loop(1, half + 1, for_partner, 0)
    for e in range(parts):
        def for_far(k, carry):
            i = lax.rem(place + k, half)
            if e == 0:
                cols_landed(0, 2 * i + core)
            value = partial_of(2 * i + core, e)
            landed(pair_in.at[e, i], pair_recv.at[e, i])
            far_out[e, i] = (value + pair_in[e, i].astype(F32)).astype(BF16)
            remote(
                far_out.at[e, i], far_in.at[e, place], far_send.at[e, i], far_recv.at[e, place],
                {"fs": 2 * i + core},
            ).start()
            return carry

        lax.fori_loop(1, half, for_far, 0)
    for e in range(parts):
        value = partial_of(f, e)
        landed(pair_in.at[e, place], pair_recv.at[e, place])
        d_act[e] = value + pair_in[e, place].astype(F32)

    landed(act_group.at[rows(partner)], act_recv.at[partner])
    forwards_landed(act_group, act_recv)
    gd_rows = gd_out.shape[1]

    def rep_copy(out, into, send, recv, c, p):
        to = lax.rem(r + p, reps)
        return remote(
            out.at[c], into.at[p - 1, c], send.at[p - 1, c], recv.at[p - 1, c], {"rep": to}
        )

    def down_step(c, carry):
        at = pl.ds(pl.multiple_of(c * gd_rows, gd_rows), gd_rows)
        for q in range(per):
            value = dot(act_group[:, at], scaled_cols[q], ((0,), (0,))) * norm_factor
            gd_out[c, :, q * cw:(q + 1) * cw] = value.astype(BF16)
        for p in range(1, reps):
            rep_copy(gd_out, gd_in, gd_send, gd_recv, c, p).start()
        return carry

    lax.fori_loop(0, gd_out.shape[0], down_step, 0)
    arriving(1, 1)
    for e in range(parts):
        total = d_act[e]
        for k in range(1, half):
            j = lax.rem(place + k, half)
            landed(far_in.at[e, j], far_recv.at[e, j])
            total = total + far_in[e, j].astype(F32)
        at = slice(e * hp, (e + 1) * hp)
        positive = jnp.maximum(pre_act[:, at].astype(F32), 0.0)
        dpre_group[e, rows(f), :] = (2.0 * positive * total * up_scale[:, at]).astype(BF16)
        group_start(dpre_group.at[e], dpre_send.at[e], dpre_recv.at[e])
        if e == 0:
            up_load.wait()
            up_bf[...] = up_f32[...].astype(BF16)
            for s in range(2, T - 1):
                arriving(1, s)
    if T > 2:
        arriving(1, T - 1)

    def send_home(ref, source):
        home, slot = lax.div(source, sub), z * sub + lax.rem(source, sub)

        @pl.when(home != z)
        def _():
            remote(
                ref, gi_in.at[slot], gi_send.at[source], gi_recv.at[slot], {"tp": home}
            ).start()

        @pl.when(home == z)
        def _():
            gi_in[slot] = ref[...]

    def input_part(source):
        value = jnp.zeros((n, w), F32)
        for e in range(parts):
            value = value + dot(
                dpre_group[e, rows(source), :], up_bf[:, e * hp:(e + 1) * hp], ((1,), (1,))
            )
        gi_out[source] = value.astype(BF16)

        if source is f:
            send_home(gi_out.at[source], f)
        else:
            remote(
                gi_out.at[source], gi_mid.at[f], mid_send.at[source], mid_recv.at[f],
                {"fs": source},
            ).start()

    def relay(source):
        landed(gi_mid.at[source], mid_recv.at[source])
        send_home(gi_mid.at[source], source)

    input_part(f)
    for e in range(parts):
        landed(dpre_group.at[e, rows(partner)], dpre_recv.at[e, partner])
    input_part(partner)
    relay(partner)

    def up_step(e):
        forwards_landed(dpre_group.at[e], dpre_recv.at[e])
        for q in range(per):
            value = dot(acts_cols[q], dpre_group[e], ((0,), (0,)))
            gu_out[e, q * cw:(q + 1) * cw, :] = (value * norm_factor).astype(BF16)
        for p in range(1, reps):
            rep_copy(gu_out, gu_in, gu_send, gu_recv, e, p).start()

    for e in range(parts):
        group_forward(dpre_group.at[e], dpre_send.at[e], dpre_recv.at[e])
        if e == 0:
            for source in range(F):
                cols_landed(1, source)
        if e < parts - 1:
            up_step(e)
    for k in range(1, half):
        input_part(lax.rem(f + 2 * k, F))
    forwards_landed(dpre_group.at[parts - 1], dpre_recv.at[parts - 1])
    for k in range(1, half):
        input_part(lax.rem(partner + 2 * k, F))
    for q in range(per):
        value = dot(acts_cols[q], dpre_group[parts - 1], ((0,), (0,)))
        gu_out[parts - 1, q * cw:(q + 1) * cw, :] = (value * norm_factor).astype(BF16)
    for p in range(1, reps):
        rep_copy(gu_out, gu_in, gu_send, gu_recv, parts - 1, p).start()
    for k in range(1, half):
        relay(lax.rem(f + 2 * k, F))
        relay(lax.rem(partner + 2 * k, F))

    def total_of(out, into, send, recv, c):
        for p in range(1, reps):
            rep_copy(out, into, send, recv, c, p).wait()
        value = out[c].astype(F32)
        for p in range(1, reps):
            value = value + into[p - 1, c].astype(F32)
        return value

    def finish_down(c, carry):
        at = pl.ds(pl.multiple_of(c * gd_rows, gd_rows), gd_rows)
        grad_down[at, :] = total_of(gd_out, gd_in, gd_send, gd_recv, c)
        return carry

    lax.fori_loop(0, gd_out.shape[0], finish_down, 0)
    for e in range(parts - 1):
        grad_up[:, e * hp:(e + 1) * hp] = total_of(gu_out, gu_in, gu_send, gu_recv, e)
    for j in range(sub):
        value = jnp.zeros((n, w), F32)
        for s in range(T):
            at = s * sub + j

            @pl.when(s != z)
            def _():
                landed(gi_in.at[at], gi_recv.at[at])

            value = value + gi_in[at].astype(F32)
        grad_input[:, j * w:(j + 1) * w] = value.astype(BF16)
    grad_up[:, (parts - 1) * hp:] = total_of(gu_out, gu_in, gu_send, gu_recv, parts - 1)

    for a in range(2):
        for block in range(T):
            for g in range(chunks):
                @pl.when((block <= z) & (z < T - 1))
                def _():
                    left_for(blocks.at[a, block, g], z_send.at[a, block, g, 0])

                @pl.when((block >= z) & (z > 0))
                def _():
                    left_for(blocks.at[a, block, g], z_send.at[a, block, g, 1])

                @pl.when(block * sub + g // per != f)
                def _():
                    left_for(blocks.at[a, block, g], col_send.at[a, block, g])
    group_sent(act_group, act_send)
    for e in range(parts):
        group_sent(dpre_group.at[e], dpre_send.at[e])
        for i in range(half):
            left_for(pair_out.at[e, i], pair_send.at[e, i])

            @pl.when(i != place)
            def _():
                left_for(far_out.at[e, i], far_send.at[e, i])
    for source in range(F):
        @pl.when(source != f)
        def _():
            left_for(gi_out.at[source], mid_send.at[source])

        @pl.when(source // sub != z)
        def _():
            left_for(gi_mid.at[source], gi_send.at[source])


def general_body(sizes, acts, cotangent, pre_act, up_store, up_scale, down_store, down_scale):
    reps, F, T = sizes
    n, d = acts.shape
    h = pre_act.shape[1]
    w = down_store.shape[1]
    half = F // 2
    cw = w // 2 if w % 256 == 0 else w
    per, chunks = w // cw, d // cw
    parts = 2 if h % 256 == 0 else 1
    hp = h // parts
    gd_rows = fitting(h, 256)
    gd_steps = h // gd_rows
    others = max(reps - 1, 1)
    sem = pltpu.SemaphoreType.DMA
    vmem, anywhere = (pl.BlockSpec(memory_space=s) for s in (pltpu.VMEM, pltpu.HBM))
    arrays = [
        ((w, h), F32), ((h, w), F32),
        ((2, T, chunks, n, cw), BF16),
        ((per, F * n, cw), BF16), ((per, F * n, cw), BF16),
        ((F * n, h), BF16), ((parts, F * n, hp), BF16),
        ((h, w), BF16), ((w, h), BF16),
        ((parts, half, n, hp), BF16), ((parts, half, n, hp), BF16),
        ((parts, half, n, hp), BF16), ((parts, half, n, hp), BF16),
        ((parts, n, hp), F32),
        ((F, n, w), BF16), ((F, n, w), BF16), ((F, n, w), BF16),
        ((gd_steps, gd_rows, w), BF16), ((others, gd_steps, gd_rows, w), BF16),
        ((parts, w, hp), BF16), ((others, parts, w, hp), BF16),
    ]
    return pl.pallas_call(
        functools.partial(general_kernel, sizes),
        out_shape=(
            jax.ShapeDtypeStruct((n, d), BF16),
            jax.ShapeDtypeStruct((w, h), F32),
            jax.ShapeDtypeStruct((h, w), F32),
        ),
        in_specs=[vmem, vmem, vmem, anywhere, vmem, anywhere, vmem],
        out_specs=(vmem, vmem, vmem),
        scratch_shapes=[pltpu.VMEM(shape, kind) for shape, kind in arrays] + [
            sem((2,)),
            sem((2, T, chunks, 2)), sem((2, T, chunks)), sem((2, T, chunks)), sem((2, F, per)),
            sem((F,)), sem((F,)), sem((parts, F)), sem((parts, F)),
            sem((parts, half)), sem((parts, half)), sem((parts, half)), sem((parts, half)),
            sem((F,)), sem((F,)), sem((F,)), sem((F,)),
            sem((others, gd_steps)), sem((others, gd_steps)),
            sem((others, parts)), sem((others, parts)),
        ],
        compiler_params=pltpu.CompilerParams(
            collective_id=0, has_side_effects=True,
            vmem_limit_bytes=60 * 1024 * 1024,
        ),
    )(
        acts, cotangent, pre_act, up_store, up_scale.reshape(1, h), down_store,
        down_scale.reshape(1, d * T),
    )


def square_kernel(
    sizes,
    acts, cotangent, pre_act, up_store, up_scale, down_store, down_scale,
    gd_out, gd_in, gu_out, gu_in, gi_in,
    acts_v, cot_v, pre_v, up_f32, up_scale_v, down_f32, down_scale_v,
    own, scaled_cols, acts_cols, pos_group, dpre_group, down_bf, up_bf,
    pair_out, pair_in, far_out, far_in, own_f32, across_f32, gi_out, gi_mid, near_in, hub_f32,
    load_sem,
    org_send, fwd_send, col_recv, act_send, act_recv, dpre_send, dpre_recv,
    pair_send, pair_recv, far_send, far_recv,
    mid_recv, near_recv, gi_send, gi_recv, relay_send,
    gd_send, gd_recv, gu_send, gu_recv,
):
    reps, F, T = sizes
    n, d = acts.shape
    h = pre_act.shape[1]
    w = down_store.shape[1]
    steps, gd_rows = gd_out.shape[0], gd_out.shape[1]
    parts, tiles, gu_rows, hp = gu_out.shape
    pieces = col_recv.shape[2]
    rp = n // pieces
    norm_factor = 1.0 / math.sqrt(n * F * reps)
    r, f, z = lax.axis_index("rep"), lax.axis_index("fs"), lax.axis_index("tp")
    core, place = lax.rem(f, 2), lax.div(f, 2)
    partner = f + 1 - 2 * core
    across = lax.rem(f + 2, F)
    corner = lax.rem(partner + 2, F)
    z_pair, z_far = z + 1 - 2 * lax.rem(z, 2), lax.rem(z + 2, T)
    mesh_ids = pl.DeviceIdType.MESH

    loads = [
        pltpu.make_async_copy(src, dst, load_sem.at[i])
        for i, (src, dst) in enumerate((
            (cotangent, cot_v), (down_scale, down_scale_v), (pre_act, pre_v),
            (down_store, down_f32), (acts, acts_v), (up_scale, up_scale_v), (up_store, up_f32),
        ))
    ]
    for load in loads:
        load.start()

    barrier = pltpu.get_barrier_semaphore()

    def greet(at, carry):
        to_f, to_z = lax.div(at, T), lax.rem(at, T)

        @pl.when((to_f != f) | (to_z != z))
        def _():
            pl.semaphore_signal(
                barrier, inc=1, device_id={"fs": to_f, "tp": to_z}, device_id_type=mesh_ids
            )

        return carry

    lax.fori_loop(0, F * T, greet, 0)
    for p in range(1, reps):
        pl.semaphore_signal(
            barrier, inc=1, device_id={"rep": lax.rem(r + p, reps)}, device_id_type=mesh_ids
        )

    def rows(at):
        return pl.ds(pl.multiple_of(at * n, n), n)

    def piece(at, p):
        return pl.ds(pl.multiple_of(at * n + p * rp, rp), rp)

    def remote(src, dst, send, recv, where):
        return pltpu.make_async_remote_copy(
            src_ref=src, dst_ref=dst, send_sem=send, recv_sem=recv,
            device_id=where, device_id_type=mesh_ids,
        )

    def landed(ref, recv):
        remote(ref, ref, recv, recv, {"fs": partner}).wait_recv()

    def left_for(ref, send):
        remote(ref, ref, send, send, {"fs": partner}).wait_send()

    cols = (scaled_cols, acts_cols)
    sources = (own, acts_v)
    same = lax.div(z, 2) == place
    direct = (z == f) | (z_far == f)
    home, hub, near = z == f, z_far == f, z_pair == f
    rises = (z > f) & (z < T - 1)
    falls = (z < f) & (z > 0)

    def originate(a, k, p, where):
        at = pl.ds(p * rp, rp)
        remote(
            sources[a].at[at], cols[a].at[piece(f, p)],
            org_send.at[a, k, p], col_recv.at[a, f, p], where,
        ).start()

    def originate_line(a):
        @pl.when(same)
        def _():
            for p in range(pieces):
                @pl.when(z < T - 1)
                def _():
                    originate(a, 1, p, {"fs": z, "tp": z + 1})

                @pl.when(z > 0)
                def _():
                    originate(a, 2, p, {"fs": z, "tp": z - 1})

                @pl.when(z != f)
                def _():
                    originate(a, 0, p, {"fs": z})

            @pl.when(z == f)
            def _():
                cols[a][rows(f), :] = sources[a][...]

    def spread_line(a):
        @pl.when(same)
        def _():
            for p in range(pieces):
                for k in range(1, T):
                    @pl.when(z + k < T)
                    def _():
                        originate(a, T + k, p, {"fs": z, "tp": z + k})

                    @pl.when(z - k >= 0)
                    def _():
                        originate(a, 1 + k, p, {"fs": z, "tp": z - k})

                @pl.when(z != f)
                def _():
                    originate(a, 0, p, {"fs": z})

            @pl.when(z == f)
            def _():
                cols[a][rows(f), :] = sources[a][...]

    def originate_cross(a):
        @pl.when(jnp.logical_not(same))
        def _():
            for p in range(pieces):
                originate(a, 1, p, {"fs": z, "tp": z_far})
                originate(a, 0, p, {"fs": z})

    def pass_on(a, source, p, to):
        ref = cols[a].at[piece(source, p)]
        landed(ref, col_recv.at[a, source, p])
        remote(ref, ref, fwd_send.at[a, source, p], col_recv.at[a, source, p], {"tp": to}).start()

    def cross_forward(a, p):
        for source in (across, corner):
            pass_on(a, source, p, z_pair)

    def line_forward(a, p):
        @pl.when(rises)
        def _():
            for source in (f, partner):
                pass_on(a, source, p, z + 1)

        @pl.when(falls)
        def _():
            for source in (f, partner):
                pass_on(a, source, p, z - 1)

    def cross_rest(a, p):
        for source in (across, corner):
            landed(cols[a].at[piece(source, p)], col_recv.at[a, source, p])

    def line_landed(a, p):
        @pl.when(z != f)
        def _():
            landed(cols[a].at[piece(f, p)], col_recv.at[a, f, p])

        landed(cols[a].at[piece(partner, p)], col_recv.at[a, partner, p])

    def line_rest(a, p):
        @pl.when(jnp.logical_not(rises | falls) & (z != f))
        def _():
            landed(cols[a].at[piece(f, p)], col_recv.at[a, f, p])

        @pl.when(jnp.logical_not(rises | falls))
        def _():
            landed(cols[a].at[piece(partner, p)], col_recv.at[a, partner, p])

    def act_cols(c):
        return pl.ds(pl.multiple_of(c * gd_rows, gd_rows), gd_rows)

    def act_send_to(source, c, k, where):
        ref = pos_group.at[rows(source), act_cols(c)]
        remote(ref, ref, act_send.at[k, c], act_recv.at[source, c], where).start()

    def act_landed(source, c):
        landed(pos_group.at[rows(source), act_cols(c)], act_recv.at[source, c])

    def act_forward(c):
        act_landed(across, c)
        act_send_to(across, c, 2, {"fs": partner})

    loads[0].wait()
    loads[1].wait()
    scale = down_scale_v[:, pl.ds(pl.multiple_of(z * d, d), d)]
    own[...] = (cot_v[...].astype(F32) * scale).astype(BF16)
    pl.semaphore_wait(barrier, F * T - 1 + reps - 1)
    originate_cross(0)
    originate_line(0)
    loads[2].wait()
    pos_group[rows(f), :] = jnp.maximum(pre_v[...].astype(F32), 0.0).astype(BF16)
    early = (steps + 1) // 2
    for c in range(early):
        act_send_to(f, c, 0, {"fs": across})

    @pl.when(jnp.logical_not(same))
    def _():
        for c in range(early, steps):
            act_send_to(f, c, 0, {"fs": across})
        gi_in[2] = jnp.zeros((n, w), BF16)

    for c in range(steps):
        act_send_to(f, c, 1, {"fs": partner})
    loads[3].wait()
    down_bf[...] = down_f32[...].astype(BF16)

    def late_act():
        for c in range(early, steps):
            act_send_to(f, c, 0, {"fs": across})

    def partial_of(target, p):
        return dot(scaled_cols[piece(target, p), :], down_bf[...], ((1,), (1,)))

    def to_partner(target, k, p):
        pair_out[k, p] = partial_of(target, p).astype(BF16)
        remote(
            pair_out.at[k, p], pair_in.at[k, p], pair_send.at[k, p], pair_recv.at[k, p],
            {"fs": partner},
        ).start()

    def far_start(p):
        value = partial_of(across, p)
        landed(pair_in.at[0, p], pair_recv.at[0, p])
        value = value + pair_in[0, p].astype(F32)
        across_f32[p] = value
        far_out[0, p] = value.astype(BF16)
        remote(
            far_out.at[0, p], far_in.at[0, p], far_send.at[0, p], far_recv.at[0, p],
            {"fs": across},
        ).start()

    for p in range(pieces):
        @pl.when(direct)
        def _():
            cross_forward(0, p)

        line_forward(0, p)

        @pl.when(direct)
        def _():
            to_partner(corner, 0, p)

    @pl.when(home)
    def _():
        late_act()

    for p in range(pieces):
        @pl.when(jnp.logical_not(direct))
        def _():
            cross_rest(0, p)
            to_partner(corner, 0, p)

        if p == 0:
            @pl.when(same & jnp.logical_not(home))
            def _():
                late_act()

        far_start(p)
    loads[4].wait()
    originate_cross(1)
    for c in range(steps):
        act_forward(c)
    for p in range(pieces):
        line_rest(0, p)
    spread_line(1)

    def rep_copy(out, into, send, recv, at, p):
        to = lax.rem(r + p, reps)
        return remote(
            out.at[at], into.at[(p - 1,) + at], send.at[(p - 1,) + at], recv.at[(p - 1,) + at],
            {"rep": to},
        )

    def down_step(c, carry):
        act_landed(partner, c)
        act_landed(corner, c)
        positive = pos_group[:, act_cols(c)].astype(F32)
        act = (positive * positive).astype(BF16)
        value = dot(act, scaled_cols[...], ((0,), (0,))) * norm_factor
        gd_out[c] = value.astype(BF16)
        for p in range(1, reps):
            rep_copy(gd_out, gd_in, gd_send, gd_recv, (c,), p).start()
        return carry

    lax.fori_loop(0, steps, down_step, 0)
    for p in range(pieces):
        to_partner(partner, 1, p)
    for p in range(pieces):
        value = partial_of(f, p)
        landed(pair_in.at[1, p], pair_recv.at[1, p])
        value = value + pair_in[1, p].astype(F32)
        own_f32[p] = value
        far_out[1, p] = value.astype(BF16)
        remote(
            far_out.at[1, p], far_in.at[1, p], far_send.at[1, p], far_recv.at[1, p],
            {"fs": across},
        ).start()
    loads[5].wait()
    loads[6].wait()
    up_bf[...] = up_f32[...].astype(BF16)

    def dpre_step(k, source, sums, p):
        landed(far_in.at[k, p], far_recv.at[k, p])
        value = sums[p] + far_in[k, p].astype(F32)
        positive = pos_group[piece(source, p), :].astype(F32)
        ref = dpre_group.at[piece(source, p)]
        ref[...] = (2.0 * positive * value * up_scale_v[...]).astype(BF16)
        remote(ref, ref, dpre_send.at[k, p], dpre_recv.at[source, p], {"fs": partner}).start()

    for p in range(pieces):
        dpre_step(0, f, own_f32, p)

        if p == 0:
            @pl.when(hub)
            def _():
                for q in range(pieces):
                    cross_forward(1, q)

    def half_rows(p):
        return pl.ds(p * rp, rp)

    def input_part(k, p):
        target = (f, partner, across, corner)[k]
        return dot(dpre_group[piece(target, p), :], up_bf[...], ((1,), (1,)))

    def input_sum(k, p, value):
        landed(near_in.at[k, half_rows(p)], near_recv.at[k, p])
        gi_out[k, half_rows(p), :] = (value + near_in[k, half_rows(p), :].astype(F32)).astype(BF16)

    def input_send(k, p, into, recv, where):
        remote(
            gi_out.at[k, half_rows(p)], into.at[half_rows(p)], gi_send.at[k, p], recv.at[p], where
        ).start()

    def own_part(k, p):
        target = (f, partner)[k]
        value = input_part(k, p)

        @pl.when(hub)
        def _():
            hub_f32[k, half_rows(p), :] = value

        @pl.when(jnp.logical_not(hub))
        def _():
            gi_out[k, half_rows(p), :] = value.astype(BF16)

        if k == 0:
            @pl.when(home)
            def _():
                gi_in[0, half_rows(p), :] = gi_out[k, half_rows(p), :]
        else:
            @pl.when(home)
            def _():
                input_send(k, p, gi_in.at[0], gi_recv.at[0], {"fs": target})

        @pl.when(near)
        def _():
            input_send(k, p, gi_in.at[2], gi_recv.at[2], {"fs": target, "tp": f})

        @pl.when(jnp.logical_not(home | near | hub))
        def _():
            input_send(k, p, near_in.at[k], near_recv.at[k], {"tp": z_pair})

    def own_sum(k, p):
        target = (f, partner)[k]

        @pl.when(hub)
        def _():
            input_sum(k, p, hub_f32[k, half_rows(p), :])
            input_send(k, p, gi_in.at[1], gi_recv.at[1], {"fs": target, "tp": f})

    def cross_part(k, p):
        value = input_part(k, p)

        @pl.when(direct)
        def _():
            hub_f32[k, half_rows(p), :] = value

        @pl.when(jnp.logical_not(direct))
        def _():
            gi_out[k, half_rows(p), :] = value.astype(BF16)
            input_send(k, p, near_in.at[k], near_recv.at[k], {"tp": z_pair})

    def cross_sum(k, p):
        target = (across, corner)[k - 2]

        @pl.when(direct)
        def _():
            input_sum(k, p, hub_f32[k, half_rows(p), :])

        @pl.when(home)
        def _():
            input_send(k, p, gi_in.at[0], gi_recv.at[0], {"fs": target})

        @pl.when(hub)
        def _():
            input_send(k, p, gi_mid, mid_recv, {"fs": target})

    for p in range(pieces):
        own_part(0, p)
    for p in range(pieces):
        landed(dpre_group.at[piece(partner, p)], dpre_recv.at[partner, p])
        own_part(1, p)

    @pl.when(home)
    def _():
        for p in range(pieces):
            cross_forward(1, p)

    def up_step(e, q):
        value = dot(
            acts_cols[:, q * gu_rows:(q + 1) * gu_rows], dpre_group[:, e * hp:(e + 1) * hp],
            ((0,), (0,)),
        )
        gu_out[e, q] = (value * norm_factor).astype(BF16)
        for p in range(1, reps):
            rep_copy(gu_out, gu_in, gu_send, gu_recv, (e, q), p).start()

    for p in range(pieces):
        dpre_step(1, across, across_f32, p)
        landed(dpre_group.at[piece(corner, p)], dpre_recv.at[corner, p])
        if p < pieces - 1:
            cross_part(2, p)
            cross_part(3, p)
    for p in range(pieces):
        @pl.when(jnp.logical_not(direct))
        def _():
            cross_rest(1, p)

        line_landed(1, p)
    for e in range(parts):
        for q in range(tiles):
            up_step(e, q)
    cross_part(2, pieces - 1)
    cross_part(3, pieces - 1)
    for p in range(pieces):
        for k in range(2, 4):
            cross_sum(k, p)
    for p in range(pieces):
        for k in range(2):
            own_sum(k, p)

    relays = lax.div(z_far, 2) != place
    for p in range(pieces):
        @pl.when(relays)
        def _():
            ref = gi_mid.at[half_rows(p)]
            landed(ref, mid_recv.at[p])
            remote(
                ref, gi_in.at[1, half_rows(p)], relay_send.at[p], gi_recv.at[1, p], {"tp": z_far}
            ).start()

    for p in range(1, reps):
        for c in range(steps):
            rep_copy(gd_out, gd_in, gd_send, gd_recv, (c,), p).wait()
    for p in range(pieces):
        @pl.when(jnp.logical_not(home))
        def _():
            landed(gi_in.at[0, half_rows(p)], gi_recv.at[0, p])

        landed(gi_in.at[1, half_rows(p)], gi_recv.at[1, p])

        @pl.when(same)
        def _():
            landed(gi_in.at[2, half_rows(p)], gi_recv.at[2, p])

    for p in range(pieces):
        for a in range(2):
            @pl.when(same & (z != f) | jnp.logical_not(same))
            def _():
                left_for(own.at[half_rows(p)], org_send.at[a, 0, p])

            @pl.when(direct)
            def _():
                for source in (across, corner):
                    left_for(own.at[half_rows(p)], fwd_send.at[a, source, p])

        @pl.when(jnp.logical_not(same))
        def _():
            for a in range(2):
                left_for(own.at[half_rows(p)], org_send.at[a, 1, p])

        @pl.when(same & (z < T - 1))
        def _():
            left_for(own.at[half_rows(p)], org_send.at[0, 1, p])

        @pl.when(same & (z > 0))
        def _():
            left_for(own.at[half_rows(p)], org_send.at[0, 2, p])

        @pl.when(rises | falls)
        def _():
            for source in (f, partner):
                left_for(own.at[half_rows(p)], fwd_send.at[0, source, p])

        for k in range(1, T):
            @pl.when(same & (z + k < T))
            def _():
                left_for(own.at[half_rows(p)], org_send.at[1, T + k, p])

            @pl.when(same & (z - k >= 0))
            def _():
                left_for(own.at[half_rows(p)], org_send.at[1, 1 + k, p])

        @pl.when(jnp.logical_not(home))
        def _():
            left_for(own.at[half_rows(p)], gi_send.at[0, p])

        for k in range(1, 4):
            left_for(own.at[half_rows(p)], gi_send.at[k, p])

        @pl.when(relays)
        def _():
            left_for(own.at[half_rows(p)], relay_send.at[p])

        for k in range(2):
            left_for(dpre_group.at[piece(f, p)], dpre_send.at[k, p])
            left_for(pair_out.at[k, p], pair_send.at[k, p])
            left_for(far_out.at[k, p], far_send.at[k, p])
    for k in range(3):
        for c in range(steps):
            left_for(pos_group.at[rows(f), act_cols(c)], act_send.at[k, c])
    for p in range(1, reps):
        for e in range(parts):
            for q in range(tiles):
                rep_copy(gu_out, gu_in, gu_send, gu_recv, (e, q), p).wait()


def finish_kernel(
    gd_out, gd_in, gu_out, gu_in, gi_in, grad_input, grad_up, grad_down,
    gi_v, gu_v, gd_v, gi_sem, gu_sem, gd_sem,
):
    others = gd_in.shape[0]
    steps, gd_rows = gd_out.shape[0], gd_out.shape[1]
    parts, tiles, gu_rows, hp = gu_out.shape
    copies = []

    def leave(src, dst, sem):
        copies.append(pltpu.make_async_copy(src, dst, sem))
        copies[-1].start()

    for c in range(steps):
        value = gd_out[c].astype(F32)
        for p in range(others):
            value = value + gd_in[p, c].astype(F32)
        gd_v[c] = value
        leave(gd_v.at[c], grad_down.at[pl.ds(c * gd_rows, gd_rows)], gd_sem.at[c])
    for e in range(parts):
        for q in range(tiles):
            value = gu_out[e, q].astype(F32)
            for p in range(others):
                value = value + gu_in[p, e, q].astype(F32)
            gu_v[e, q] = value
            at = (pl.ds(q * gu_rows, gu_rows), pl.ds(e * hp, hp))
            leave(gu_v.at[e, q], grad_up.at[at], gu_sem.at[e, q])
    value = gi_in[0].astype(F32)
    for s in range(1, gi_in.shape[0]):
        value = value + gi_in[s].astype(F32)
    gi_v[...] = value.astype(BF16)
    leave(gi_v, grad_input, gi_sem.at[0])
    for copy in copies:
        copy.wait()


def square_body(sizes, acts, cotangent, pre_act, up_store, up_scale, down_store, down_scale):
    reps, F, T = sizes
    n, d = acts.shape
    h = pre_act.shape[1]
    w = down_store.shape[1]
    parts = 2 if h % 256 == 0 else 1
    pieces = 2 if n % 32 == 0 else 1
    tiles = 2 if w % 256 == 0 else 1
    hp, rp = h // parts, n // pieces
    gd_rows = fitting(h, 256)
    steps = h // gd_rows
    others = reps - 1
    sem = pltpu.SemaphoreType.DMA
    vmem, hbm = (pl.BlockSpec(memory_space=s) for s in (pltpu.VMEM, pltpu.HBM))
    shared = [
        (steps, gd_rows, w), (others, steps, gd_rows, w),
        (parts, tiles, w // tiles, hp), (others, parts, tiles, w // tiles, hp),
        (3, n, w),
    ]
    arrays = [
        ((n, d), BF16), ((n, d), BF16), ((n, h), BF16),
        ((w, h), F32), ((1, h), F32), ((h, w), F32), ((1, d * T), F32),
        ((n, d), BF16), ((F * n, w), BF16), ((F * n, w), BF16),
        ((F * n, h), BF16), ((F * n, h), BF16),
        ((h, w), BF16), ((w, h), BF16),
        ((2, pieces, rp, h), BF16), ((2, pieces, rp, h), BF16),
        ((2, pieces, rp, h), BF16), ((2, pieces, rp, h), BF16),
        ((pieces, rp, h), F32), ((pieces, rp, h), F32),
        ((F, n, w), BF16), ((n, w), BF16), ((F, n, w), BF16), ((F, n, w), F32),
    ]
    moved = pl.pallas_call(
        functools.partial(square_kernel, sizes),
        out_shape=tuple(jax.ShapeDtypeStruct(shape, BF16) for shape in shared),
        in_specs=[hbm] * 7,
        out_specs=(vmem,) * len(shared),
        scratch_shapes=[pltpu.VMEM(shape, kind) for shape, kind in arrays] + [
            sem((7,)),
            sem((2, 2 * T, pieces)), sem((2, F, pieces)), sem((2, F, pieces)),
            sem((3, steps)), sem((F, steps)), sem((2, pieces)), sem((F, pieces)),
            sem((2, pieces)), sem((2, pieces)), sem((2, pieces)), sem((2, pieces)),
            sem((pieces,)), sem((F, pieces)), sem((F, pieces)), sem((3, pieces)), sem((pieces,)),
            sem((others, steps)), sem((others, steps)),
            sem((others, parts, tiles)), sem((others, parts, tiles)),
        ],
        compiler_params=pltpu.CompilerParams(
            collective_id=0, has_side_effects=True,
            vmem_limit_bytes=40 * 1024 * 1024,
        ),
    )(*(
        pltpu.with_memory_space_constraint(array, pltpu.HBM)
        for array in (
            acts, cotangent, pre_act, up_store, up_scale.reshape(1, h), down_store,
            down_scale.reshape(1, d * T),
        )
    ))
    return pl.pallas_call(
        finish_kernel,
        out_shape=(
            jax.ShapeDtypeStruct((n, d), BF16),
            jax.ShapeDtypeStruct((w, h), F32),
            jax.ShapeDtypeStruct((h, w), F32),
        ),
        in_specs=[vmem] * len(shared),
        out_specs=(hbm,) * 3,
        scratch_shapes=[
            pltpu.VMEM((n, d), BF16),
            pltpu.VMEM((parts, tiles, w // tiles, hp), F32),
            pltpu.VMEM((steps, gd_rows, w), F32),
            sem((1,)), sem((parts, tiles)), sem((steps,)),
        ],
        compiler_params=pltpu.CompilerParams(vmem_limit_bytes=12 * 1024 * 1024),
    )(*moved)


def body(sizes, *arrays):
    reps, F, T = sizes
    square = F == T and F == 2 * 2 and reps > 1
    return (square_body if square else general_body)(sizes, *arrays)


def solution(mesh):
    sizes = (mesh.shape["rep"], mesh.shape["fs"], mesh.shape["tp"])
    return jax.shard_map(
        functools.partial(body, sizes),
        mesh=mesh,
        in_specs=(
            P(("rep", "fs"), "tp"),
            P(("rep", "fs"), "tp"),
            P(("rep", "fs"), "tp"),
            P("fs", "tp"),
            P("tp"),
            P("tp", "fs"),
            P(),
        ),
        out_specs=(P(("rep", "fs"), "tp"), P("fs", "tp"), P("tp", "fs")),
        check_vma=False,
    )
```

```python
import functools
import math

import jax
import jax.numpy as jnp
from jax import lax
from jax.experimental import pallas as pl
from jax.experimental.pallas import tpu as pltpu
from jax.sharding import PartitionSpec as P

F32, BF16 = jnp.float32, jnp.bfloat16


def dot(left, right, dims):
    return lax.dot_general(left, right, (dims, ((), ())), preferred_element_type=F32)


def fitting(size, most):
    return most if size % most == 0 else size


def general_kernel(
    sizes,
    acts, cotangent, pre_act, up_store, up_scale, down_store, down_scale,
    grad_input, grad_up, grad_down,
    up_f32, down_f32,
    blocks, scaled_cols, acts_cols, act_group, dpre_group, down_bf, up_bf,
    pair_out, pair_in, far_out, far_in, d_act, gi_out, gi_mid, gi_in,
    gd_out, gd_in, gu_out, gu_in,
    load_sem,
    z_send, z_recv, col_send, col_recv, act_send, act_recv, dpre_send, dpre_recv,
    pair_send, pair_recv, far_send, far_recv, mid_send, mid_recv, gi_send, gi_recv,
    gd_send, gd_recv, gu_send, gu_recv,
):
    reps, F, T = sizes
    n, d = acts.shape
    h = pre_act.shape[1]
    w = down_store.shape[1]
    half, sub = F // 2, F // T
    chunks, cw = blocks.shape[2], blocks.shape[4]
    per = w // cw
    parts, hp = dpre_group.shape[0], dpre_group.shape[2]
    norm_factor = 1.0 / math.sqrt(n * F * reps)
    r, f, z = lax.axis_index("rep"), lax.axis_index("fs"), lax.axis_index("tp")
    core, place = lax.rem(f, 2), lax.div(f, 2)
    partner = f + 1 - 2 * core
    mesh_ids = pl.DeviceIdType.MESH

    down_load = pltpu.make_async_copy(down_store, down_f32, load_sem.at[0])
    up_load = pltpu.make_async_copy(up_store, up_f32, load_sem.at[1])
    down_load.start()
    up_load.start()

    barrier = pltpu.get_barrier_semaphore()

    def greet(at, carry):
        to_f, to_z = lax.div(at, T), lax.rem(at, T)

        @pl.when((to_f != f) | (to_z != z))
        def _():
            pl.semaphore_signal(
                barrier, inc=1, device_id={"fs": to_f, "tp": to_z}, device_id_type=mesh_ids
            )

        return carry

    lax.fori_loop(0, F * T, greet, 0)
    for p in range(1, reps):
        pl.semaphore_signal(
            barrier, inc=1, device_id={"rep": lax.rem(r + p, reps)}, device_id_type=mesh_ids
        )

    def rows(at):
        return pl.ds(pl.multiple_of(at * n, n), n)

    def remote(src, dst, send, recv, where):
        return pltpu.make_async_remote_copy(
            src_ref=src, dst_ref=dst, send_sem=send, recv_sem=recv,
            device_id=where, device_id_type=mesh_ids,
        )

    def landed(ref, recv):
        remote(ref, ref, recv, recv, {"fs": partner}).wait_recv()

    def left_for(ref, send):
        remote(ref, ref, send, send, {"fs": partner}).wait_send()

    cols = (scaled_cols, acts_cols)

    def pass_on(a, block, g, way):
        @pl.when((z < T - 1) if way == 0 else (z > 0))
        def _():
            ref = blocks.at[a, block, g]
            to = z + 1 if way == 0 else z - 1
            remote(ref, ref, z_send.at[a, block, g, way], z_recv.at[a, block, g], {"tp": to}).start()

    def spread(a, block, g):
        target, q = block * sub + g // per, g % per

        @pl.when(target != f)
        def _():
            remote(
                blocks.at[a, block, g], cols[a].at[q, rows(f)],
                col_send.at[a, block, g], col_recv.at[a, f, q], {"fs": target},
            ).start()

        @pl.when(target == f)
        def _():
            cols[a][q, rows(f), :] = blocks[a, block, g]

    def own_block(a):
        for g in range(chunks):
            pass_on(a, z, g, 0)
            pass_on(a, z, g, 1)
        for g in range(chunks):
            spread(a, z, g)

    def arriving(a, s):
        for g in range(chunks):
            @pl.when(z - s >= 0)
            def _():
                landed(blocks.at[a, z - s, g], z_recv.at[a, z - s, g])
                pass_on(a, z - s, g, 0)
                spread(a, z - s, g)

            @pl.when(z + s <= T - 1)
            def _():
                landed(blocks.at[a, z + s, g], z_recv.at[a, z + s, g])
                pass_on(a, z + s, g, 1)
                spread(a, z + s, g)

    def cols_landed(a, source):
        @pl.when(source != f)
        def _():
            for q in range(per):
                landed(cols[a].at[q, rows(source)], col_recv.at[a, source, q])

    def group_start(group, send, recv):
        ref = group.at[rows(f)]
        for k in range(1, half):
            to = lax.rem(f + 2 * k, F)
            remote(ref, ref, send.at[k], recv.at[f], {"fs": to}).start()
        remote(ref, ref, send.at[0], recv.at[f], {"fs": partner}).start()

    def group_forward(group, send, recv):
        for k in range(1, half):
            source = lax.rem(f - 2 * k + F, F)
            ref = group.at[rows(source)]
            landed(ref, recv.at[source])
            remote(ref, ref, send.at[half - 1 + k], recv.at[source], {"fs": partner}).start()

    def forwards_landed(group, recv):
        for k in range(1, half):
            source = lax.rem(partner + 2 * k, F)
            landed(group.at[rows(source)], recv.at[source])

    def group_sent(group, send):
        for k in range(F - 1):
            left_for(group.at[rows(f)], send.at[k])

    scale = down_scale[:, pl.ds(pl.multiple_of(z * d, d), d)]
    scaled = (cotangent[...].astype(F32) * scale).astype(BF16)
    for g in range(chunks):
        blocks[0, z, g] = scaled[:, g * cw:(g + 1) * cw]
    positive = jnp.maximum(pre_act[...].astype(F32), 0.0)
    act_group[rows(f), :] = (positive * positive).astype(BF16)
    pl.semaphore_wait(barrier, F * T - 1 + reps - 1)
    own_block(0)
    group_start(act_group, act_send, act_recv)
    for g in range(chunks):
        blocks[1, z, g] = acts[:, g * cw:(g + 1) * cw]
    down_load.wait()
    down_bf[...] = down_f32[...].astype(BF16)
    for s in range(1, T):
        if s == T - 1:
            group_forward(act_group, act_send, act_recv)
        arriving(0, s)
    own_block(1)

    def partial_of(target, e):
        value = jnp.zeros((n, hp), F32)
        for q in range(per):
            value = value + dot(
                scaled_cols[q, rows(target), :],
                down_bf[e * hp:(e + 1) * hp, q * cw:(q + 1) * cw], ((1,), (1,)),
            )
        return value

    for e in range(parts):
        def for_partner(k, carry):
            i = lax.rem(place + k, half)
            if e == 0:
                cols_landed(0, 2 * i + 1 - core)
            pair_out[e, i] = partial_of(2 * i + 1 - core, e).astype(BF16)
            remote(
                pair_out.at[e, i], pair_in.at[e, i], pair_send.at[e, i], pair_recv.at[e, i],
                {"fs": partner},
            ).start()
            return carry

        lax.fori_loop(1, half + 1, for_partner, 0)
    for e in range(parts):
        def for_far(k, carry):
            i = lax.rem(place + k, half)
            if e == 0:
                cols_landed(0, 2 * i + core)
            value = partial_of(2 * i + core, e)
            landed(pair_in.at[e, i], pair_recv.at[e, i])
            far_out[e, i] = (value + pair_in[e, i].astype(F32)).astype(BF16)
            remote(
                far_out.at[e, i], far_in.at[e, place], far_send.at[e, i], far_recv.at[e, place],
                {"fs": 2 * i + core},
            ).start()
            return carry

        lax.fori_loop(1, half, for_far, 0)
    for e in range(parts):
        value = partial_of(f, e)
        landed(pair_in.at[e, place], pair_recv.at[e, place])
        d_act[e] = value + pair_in[e, place].astype(F32)

    landed(act_group.at[rows(partner)], act_recv.at[partner])
    forwards_landed(act_group, act_recv)
    gd_rows = gd_out.shape[1]

    def rep_copy(out, into, send, recv, c, p):
        to = lax.rem(r + p, reps)
        return remote(
            out.at[c], into.at[p - 1, c], send.at[p - 1, c], recv.at[p - 1, c], {"rep": to}
        )

    def down_step(c, carry):
        at = pl.ds(pl.multiple_of(c * gd_rows, gd_rows), gd_rows)
        for q in range(per):
            value = dot(act_group[:, at], scaled_cols[q], ((0,), (0,))) * norm_factor
            gd_out[c, :, q * cw:(q + 1) * cw] = value.astype(BF16)
        for p in range(1, reps):
            rep_copy(gd_out, gd_in, gd_send, gd_recv, c, p).start()
        return carry

    lax.fori_loop(0, gd_out.shape[0], down_step, 0)
    arriving(1, 1)
    for e in range(parts):
        total = d_act[e]
        for k in range(1, half):
            j = lax.rem(place + k, half)
            landed(far_in.at[e, j], far_recv.at[e, j])
            total = total + far_in[e, j].astype(F32)
        at = slice(e * hp, (e + 1) * hp)
        positive = jnp.maximum(pre_act[:, at].astype(F32), 0.0)
        dpre_group[e, rows(f), :] = (2.0 * positive * total * up_scale[:, at]).astype(BF16)
        group_start(dpre_group.at[e], dpre_send.at[e], dpre_recv.at[e])
        if e == 0:
            up_load.wait()
            up_bf[...] = up_f32[...].astype(BF16)
            for s in range(2, T - 1):
                arriving(1, s)
    if T > 2:
        arriving(1, T - 1)

    def send_home(ref, source):
        home, slot = lax.div(source, sub), z * sub + lax.rem(source, sub)

        @pl.when(home != z)
        def _():
            remote(
                ref, gi_in.at[slot], gi_send.at[source], gi_recv.at[slot], {"tp": home}
            ).start()

        @pl.when(home == z)
        def _():
            gi_in[slot] = ref[...]

    def input_part(source):
        value = jnp.zeros((n, w), F32)
        for e in range(parts):
            value = value + dot(
                dpre_group[e, rows(source), :], up_bf[:, e * hp:(e + 1) * hp], ((1,), (1,))
            )
        gi_out[source] = value.astype(BF16)

        if source is f:
            send_home(gi_out.at[source], f)
        else:
            remote(
                gi_out.at[source], gi_mid.at[f], mid_send.at[source], mid_recv.at[f],
                {"fs": source},
            ).start()

    def relay(source):
        landed(gi_mid.at[source], mid_recv.at[source])
        send_home(gi_mid.at[source], source)

    input_part(f)
    for e in range(parts):
        landed(dpre_group.at[e, rows(partner)], dpre_recv.at[e, partner])
    input_part(partner)
    relay(partner)

    def up_step(e):
        forwards_landed(dpre_group.at[e], dpre_recv.at[e])
        for q in range(per):
            value = dot(acts_cols[q], dpre_group[e], ((0,), (0,)))
            gu_out[e, q * cw:(q + 1) * cw, :] = (value * norm_factor).astype(BF16)
        for p in range(1, reps):
            rep_copy(gu_out, gu_in, gu_send, gu_recv, e, p).start()

    for e in range(parts):
        group_forward(dpre_group.at[e], dpre_send.at[e], dpre_recv.at[e])
        if e == 0:
            for source in range(F):
                cols_landed(1, source)
        if e < parts - 1:
            up_step(e)
    for k in range(1, half):
        input_part(lax.rem(f + 2 * k, F))
    forwards_landed(dpre_group.at[parts - 1], dpre_recv.at[parts - 1])
    for k in range(1, half):
        input_part(lax.rem(partner + 2 * k, F))
    for q in range(per):
        value = dot(acts_cols[q], dpre_group[parts - 1], ((0,), (0,)))
        gu_out[parts - 1, q * cw:(q + 1) * cw, :] = (value * norm_factor).astype(BF16)
    for p in range(1, reps):
        rep_copy(gu_out, gu_in, gu_send, gu_recv, parts - 1, p).start()
    for k in range(1, half):
        relay(lax.rem(f + 2 * k, F))
        relay(lax.rem(partner + 2 * k, F))

    def total_of(out, into, send, recv, c):
        for p in range(1, reps):
            rep_copy(out, into, send, recv, c, p).wait()
        value = out[c].astype(F32)
        for p in range(1, reps):
            value = value + into[p - 1, c].astype(F32)
        return value

    def finish_down(c, carry):
        at = pl.ds(pl.multiple_of(c * gd_rows, gd_rows), gd_rows)
        grad_down[at, :] = total_of(gd_out, gd_in, gd_send, gd_recv, c)
        return carry

    lax.fori_loop(0, gd_out.shape[0], finish_down, 0)
    for e in range(parts - 1):
        grad_up[:, e * hp:(e + 1) * hp] = total_of(gu_out, gu_in, gu_send, gu_recv, e)
    for j in range(sub):
        value = jnp.zeros((n, w), F32)
        for s in range(T):
            at = s * sub + j

            @pl.when(s != z)
            def _():
                landed(gi_in.at[at], gi_recv.at[at])

            value = value + gi_in[at].astype(F32)
        grad_input[:, j * w:(j + 1) * w] = value.astype(BF16)
    grad_up[:, (parts - 1) * hp:] = total_of(gu_out, gu_in, gu_send, gu_recv, parts - 1)

    for a in range(2):
        for block in range(T):
            for g in range(chunks):
                @pl.when((block <= z) & (z < T - 1))
                def _():
                    left_for(blocks.at[a, block, g], z_send.at[a, block, g, 0])

                @pl.when((block >= z) & (z > 0))
                def _():
                    left_for(blocks.at[a, block, g], z_send.at[a, block, g, 1])

                @pl.when(block * sub + g // per != f)
                def _():
                    left_for(blocks.at[a, block, g], col_send.at[a, block, g])
    group_sent(act_group, act_send)
    for e in range(parts):
        group_sent(dpre_group.at[e], dpre_send.at[e])
        for i in range(half):
            left_for(pair_out.at[e, i], pair_send.at[e, i])

            @pl.when(i != place)
            def _():
                left_for(far_out.at[e, i], far_send.at[e, i])
    for source in range(F):
        @pl.when(source != f)
        def _():
            left_for(gi_out.at[source], mid_send.at[source])

        @pl.when(source // sub != z)
        def _():
            left_for(gi_mid.at[source], gi_send.at[source])


def general_body(sizes, acts, cotangent, pre_act, up_store, up_scale, down_store, down_scale):
    reps, F, T = sizes
    n, d = acts.shape
    h = pre_act.shape[1]
    w = down_store.shape[1]
    half = F // 2
    cw = w // 2 if w % 256 == 0 else w
    per, chunks = w // cw, d // cw
    parts = 2 if h % 256 == 0 else 1
    hp = h // parts
    gd_rows = fitting(h, 256)
    gd_steps = h // gd_rows
    others = max(reps - 1, 1)
    sem = pltpu.SemaphoreType.DMA
    vmem, anywhere = (pl.BlockSpec(memory_space=s) for s in (pltpu.VMEM, pltpu.HBM))
    arrays = [
        ((w, h), F32), ((h, w), F32),
        ((2, T, chunks, n, cw), BF16),
        ((per, F * n, cw), BF16), ((per, F * n, cw), BF16),
        ((F * n, h), BF16), ((parts, F * n, hp), BF16),
        ((h, w), BF16), ((w, h), BF16),
        ((parts, half, n, hp), BF16), ((parts, half, n, hp), BF16),
        ((parts, half, n, hp), BF16), ((parts, half, n, hp), BF16),
        ((parts, n, hp), F32),
        ((F, n, w), BF16), ((F, n, w), BF16), ((F, n, w), BF16),
        ((gd_steps, gd_rows, w), BF16), ((others, gd_steps, gd_rows, w), BF16),
        ((parts, w, hp), BF16), ((others, parts, w, hp), BF16),
    ]
    return pl.pallas_call(
        functools.partial(general_kernel, sizes),
        out_shape=(
            jax.ShapeDtypeStruct((n, d), BF16),
            jax.ShapeDtypeStruct((w, h), F32),
            jax.ShapeDtypeStruct((h, w), F32),
        ),
        in_specs=[vmem, vmem, vmem, anywhere, vmem, anywhere, vmem],
        out_specs=(vmem, vmem, vmem),
        scratch_shapes=[pltpu.VMEM(shape, kind) for shape, kind in arrays] + [
            sem((2,)),
            sem((2, T, chunks, 2)), sem((2, T, chunks)), sem((2, T, chunks)), sem((2, F, per)),
            sem((F,)), sem((F,)), sem((parts, F)), sem((parts, F)),
            sem((parts, half)), sem((parts, half)), sem((parts, half)), sem((parts, half)),
            sem((F,)), sem((F,)), sem((F,)), sem((F,)),
            sem((others, gd_steps)), sem((others, gd_steps)),
            sem((others, parts)), sem((others, parts)),
        ],
        compiler_params=pltpu.CompilerParams(
            collective_id=0, has_side_effects=True,
            vmem_limit_bytes=60 * 1024 * 1024,
        ),
    )(
        acts, cotangent, pre_act, up_store, up_scale.reshape(1, h), down_store,
        down_scale.reshape(1, d * T),
    )


def square_kernel(
    sizes,
    acts, cotangent, pre_act, up_store, up_scale, down_store, down_scale,
    gd_out, gd_in, gu_out, gu_in, gi_in,
    acts_v, cot_v, pre_v, up_f32, up_scale_v, down_f32, down_scale_v,
    own, scaled_cols, acts_cols, pos_group, dpre_group, down_bf, up_bf,
    pair_out, pair_in, far_out, far_in, sums, gi_out, gi_mid, near_in, hub_f32,
    load_sem,
    org_send, fwd_send, col_recv, act_send, act_recv, dpre_send, dpre_recv,
    pair_send, pair_recv, far_send, far_recv,
    mid_recv, near_recv, gi_send, gi_recv, relay_send,
    gd_send, gd_recv, gu_send, gu_recv,
):
    reps, F, T = sizes
    n, d = acts.shape
    h = pre_act.shape[1]
    w = down_store.shape[1]
    steps, gd_rows = gd_out.shape[0], gd_out.shape[1]
    parts, tiles, gu_rows, hp = gu_out.shape
    pieces, strips = sums.shape[1], col_recv.shape[2]
    rp, sp = n // pieces, n // strips
    norm_factor = 1.0 / math.sqrt(n * F * reps)
    r, f, z = lax.axis_index("rep"), lax.axis_index("fs"), lax.axis_index("tp")
    core, place = lax.rem(f, 2), lax.div(f, 2)
    partner = f + 1 - 2 * core
    across = lax.rem(f + 2, F)
    corner = lax.rem(partner + 2, F)
    z_pair, z_far = z + 1 - 2 * lax.rem(z, 2), lax.rem(z + 2, T)
    mesh_ids = pl.DeviceIdType.MESH

    loads = [
        pltpu.make_async_copy(src, dst, load_sem.at[i])
        for i, (src, dst) in enumerate((
            (cotangent, cot_v), (down_scale, down_scale_v), (pre_act, pre_v),
            (down_store, down_f32), (acts, acts_v), (up_scale, up_scale_v), (up_store, up_f32),
        ))
    ]
    for load in loads:
        load.start()

    barrier = pltpu.get_barrier_semaphore()

    def greet(at, carry):
        to_f, to_z = lax.div(at, T), lax.rem(at, T)

        @pl.when((to_f != f) | (to_z != z))
        def _():
            pl.semaphore_signal(
                barrier, inc=1, device_id={"fs": to_f, "tp": to_z}, device_id_type=mesh_ids
            )

        return carry

    lax.fori_loop(0, F * T, greet, 0)
    for p in range(1, reps):
        pl.semaphore_signal(
            barrier, inc=1, device_id={"rep": lax.rem(r + p, reps)}, device_id_type=mesh_ids
        )

    def rows(at):
        return pl.ds(pl.multiple_of(at * n, n), n)

    def piece(at, p):
        return pl.ds(pl.multiple_of(at * n + p * rp, rp), rp)

    def strip(at, p):
        return pl.ds(pl.multiple_of(at * n + p * sp, sp), sp)

    def strips_of(p):
        return range(p * strips // pieces, (p + 1) * strips // pieces)

    def remote(src, dst, send, recv, where):
        return pltpu.make_async_remote_copy(
            src_ref=src, dst_ref=dst, send_sem=send, recv_sem=recv,
            device_id=where, device_id_type=mesh_ids,
        )

    def landed(ref, recv):
        remote(ref, ref, recv, recv, {"fs": partner}).wait_recv()

    def left_for(ref, send):
        remote(ref, ref, send, send, {"fs": partner}).wait_send()

    cols = (scaled_cols, acts_cols)
    sources = (own, acts_v)
    same = lax.div(z, 2) == place
    direct = (z == f) | (z_far == f)
    home, hub, near = z == f, z_far == f, z_pair == f
    rises = (z > f) & (z < T - 1)
    falls = (z < f) & (z > 0)

    def originate(a, k, p, where):
        at = pl.ds(p * sp, sp)
        remote(
            sources[a].at[at], cols[a].at[strip(f, p)],
            org_send.at[a, k, p], col_recv.at[a, f, p], where,
        ).start()

    def originate_line(a):
        @pl.when(same)
        def _():
            for p in range(strips):
                @pl.when(z < T - 1)
                def _():
                    originate(a, 1, p, {"fs": z, "tp": z + 1})

                @pl.when(z > 0)
                def _():
                    originate(a, 2, p, {"fs": z, "tp": z - 1})

                @pl.when(z != f)
                def _():
                    originate(a, 0, p, {"fs": z})

            @pl.when(z == f)
            def _():
                cols[a][rows(f), :] = sources[a][...]

    def spread_inner(a):
        @pl.when(same)
        def _():
            for p in range(strips):
                for k in range(1, T - 1):
                    @pl.when(z + k < T - 1)
                    def _():
                        originate(a, T + k, p, {"fs": z, "tp": z + k})

                    @pl.when(z - k > 0)
                    def _():
                        originate(a, 1 + k, p, {"fs": z, "tp": z - k})

    def spread_outer(a):
        @pl.when(same)
        def _():
            for p in range(strips):
                @pl.when(z == T - 2)
                def _():
                    originate(a, T + 1, p, {"fs": z, "tp": z + 1})

                @pl.when(z == 1)
                def _():
                    originate(a, 2, p, {"fs": z, "tp": z - 1})

                @pl.when(z != f)
                def _():
                    originate(a, 0, p, {"fs": z})

            @pl.when(z == f)
            def _():
                cols[a][rows(f), :] = sources[a][...]

    def originate_cross(a):
        @pl.when(jnp.logical_not(same))
        def _():
            for p in range(strips):
                originate(a, 1, p, {"fs": z, "tp": z_far})
                if a == 0:
                    originate(a, 0, p, {"fs": z})

    def pass_on(a, source, p, to):
        ref = cols[a].at[strip(source, p)]
        landed(ref, col_recv.at[a, source, p])
        remote(ref, ref, fwd_send.at[a, source, p], col_recv.at[a, source, p], {"tp": to}).start()

    def cross_forward(a, p):
        for source in (across, corner):
            pass_on(a, source, p, z_pair)

    def line_forward(a, p):
        @pl.when(rises)
        def _():
            for source in (f, partner):
                pass_on(a, source, p, z + 1)

        @pl.when(falls)
        def _():
            for source in (f, partner):
                pass_on(a, source, p, z - 1)

    def cross_rest(a, p):
        for source in (across, corner):
            landed(cols[a].at[strip(source, p)], col_recv.at[a, source, p])

    last_up, last_down = (z > f) & (z == T - 2), (z < f) & (z == 1)

    def tip_forward(a, p):
        @pl.when(last_up)
        def _():
            for source in (f, partner):
                pass_on(a, source, p, z + 1)

        @pl.when(last_down)
        def _():
            for source in (f, partner):
                pass_on(a, source, p, z - 1)

    def line_landed(a, p):
        @pl.when(jnp.logical_not(last_up | last_down) & (z != f))
        def _():
            landed(cols[a].at[strip(f, p)], col_recv.at[a, f, p])

        @pl.when(jnp.logical_not(last_up | last_down))
        def _():
            landed(cols[a].at[strip(partner, p)], col_recv.at[a, partner, p])

    def line_rest(a, p):
        @pl.when(jnp.logical_not(rises | falls) & (z != f))
        def _():
            landed(cols[a].at[strip(f, p)], col_recv.at[a, f, p])

        @pl.when(jnp.logical_not(rises | falls))
        def _():
            landed(cols[a].at[strip(partner, p)], col_recv.at[a, partner, p])

    def act_cols(c):
        return pl.ds(pl.multiple_of(c * gd_rows, gd_rows), gd_rows)

    def act_send_to(source, c, k, where):
        ref = pos_group.at[rows(source), act_cols(c)]
        remote(ref, ref, act_send.at[k, c], act_recv.at[source, c], where).start()

    def act_landed(source, c):
        landed(pos_group.at[rows(source), act_cols(c)], act_recv.at[source, c])

    def act_forward(c):
        act_landed(across, c)
        act_send_to(across, c, 2, {"fs": partner})

    loads[0].wait()
    loads[1].wait()
    scale = down_scale_v[:, pl.ds(pl.multiple_of(z * d, d), d)]
    own[...] = (cot_v[...].astype(F32) * scale).astype(BF16)
    pl.semaphore_wait(barrier, F * T - 1 + reps - 1)
    originate_cross(0)
    originate_line(0)
    loads[2].wait()
    pos_group[rows(f), :] = jnp.maximum(pre_v[...].astype(F32), 0.0).astype(BF16)
    for c in range(steps):
        act_send_to(f, c, 0, {"fs": across})

    loads[4].wait()

    @pl.when(jnp.logical_not(same))
    def _():
        for p in range(strips):
            originate(1, 0, p, {"fs": z})
        gi_in[2] = jnp.zeros((n, w), BF16)

    for c in range(steps):
        act_send_to(f, c, 1, {"fs": partner})
    loads[3].wait()
    down_bf[...] = down_f32[...].astype(BF16)

    def partial_of(target, p):
        return dot(scaled_cols[piece(target, p), :], down_bf[...], ((1,), (1,)))

    def to_partner(target, k, p):
        pair_out[k, p] = partial_of(target, p).astype(BF16)
        remote(
            pair_out.at[k, p], pair_in.at[k, p], pair_send.at[k, p], pair_recv.at[k, p],
            {"fs": partner},
        ).start()

    def chip_sum(target, k, p):
        value = partial_of(target, p)
        landed(pair_in.at[k, p], pair_recv.at[k, p])
        value = value + pair_in[k, p].astype(F32)
        sums[k, p] = value
        for e in range(parts):
            far_out[k, e, p] = value[:, e * hp:(e + 1) * hp].astype(BF16)

    def far_start(k, e, p):
        remote(
            far_out.at[k, e, p], far_in.at[k, e, p], far_send.at[k, e, p], far_recv.at[k, e, p],
            {"fs": across},
        ).start()

    for p in range(pieces):
        for t in strips_of(p):
            @pl.when(direct)
            def _():
                cross_forward(0, t)

            line_forward(0, t)

        @pl.when(direct)
        def _():
            to_partner(corner, 0, p)

    def rep_copy(out, into, send, recv, at, p):
        to = lax.rem(r + p, reps)
        return remote(
            out.at[at], into.at[(p - 1,) + at], send.at[(p - 1,) + at], recv.at[(p - 1,) + at],
            {"rep": to},
        )

    def down_step(c, carry):
        act_landed(partner, c)
        act_landed(corner, c)
        positive = pos_group[:, act_cols(c)].astype(F32)
        act = (positive * positive).astype(BF16)
        value = dot(act, scaled_cols[...], ((0,), (0,))) * norm_factor
        gd_out[c] = value.astype(BF16)
        for p in range(1, reps):
            rep_copy(gd_out, gd_in, gd_send, gd_recv, (c,), p).start()
        return carry

    def forward_and_down(c, carry):
        act_forward(c)
        return down_step(c, carry)

    spread_inner(1)

    @pl.when(direct)
    def _():
        for p in range(strips):
            line_rest(0, p)
        lax.fori_loop(0, steps, forward_and_down, 0)

    half_steps = steps // 2
    for p in range(pieces):
        @pl.when(jnp.logical_not(direct))
        def _():
            for c in range(half_steps * p, steps if p == pieces - 1 else half_steps):
                act_forward(c)
            for t in strips_of(p):
                cross_rest(0, t)
            to_partner(corner, 0, p)

        chip_sum(across, 0, p)
        for e in range(parts):
            far_start(0, e, p)
    originate_cross(1)
    spread_outer(1)

    @pl.when(jnp.logical_not(direct))
    def _():
        for p in range(strips):
            line_rest(0, p)
        lax.fori_loop(0, steps, down_step, 0)


    for p in range(strips):
        tip_forward(1, p)

    @pl.when(home)
    def _():
        for p in range(strips):
            cross_forward(1, p)

    for p in range(pieces):
        to_partner(partner, 1, p)
    for p in range(pieces):
        chip_sum(f, 1, p)
    for e in range(parts):
        for p in range(pieces):
            far_start(1, e, p)
    loads[5].wait()
    loads[6].wait()
    up_bf[...] = up_f32[...].astype(BF16)

    def hidden(e):
        return pl.ds(e * hp, hp)

    def dpre_step(k, source, e, p):
        landed(far_in.at[k, e, p], far_recv.at[k, e, p])
        at = hidden(e)
        value = sums[1 - k, p, :, at] + far_in[k, e, p].astype(F32)
        positive = pos_group[piece(source, p), at].astype(F32)
        ref = dpre_group.at[piece(source, p), at]
        ref[...] = (2.0 * positive * value * up_scale_v[:, at]).astype(BF16)
        remote(ref, ref, dpre_send.at[k, e, p], dpre_recv.at[e, source, p], {"fs": partner}).start()

    def dpre_landed(source, e, p):
        landed(dpre_group.at[piece(source, p), hidden(e)], dpre_recv.at[e, source, p])

    @pl.when(hub)
    def _():
        for p in range(strips):
            cross_forward(1, p)

    for p in range(pieces):
        for e in range(parts):
            dpre_step(0, f, e, p)

    def half_rows(p):
        return pl.ds(p * rp, rp)

    def input_part(k, p):
        target = (f, partner, across, corner)[k]
        return dot(dpre_group[piece(target, p), :], up_bf[...], ((1,), (1,)))

    def input_sum(k, p, value):
        landed(near_in.at[k, half_rows(p)], near_recv.at[k, p])
        gi_out[k, half_rows(p), :] = (value + near_in[k, half_rows(p), :].astype(F32)).astype(BF16)

    def input_send(k, p, into, recv, where):
        remote(
            gi_out.at[k, half_rows(p)], into.at[half_rows(p)], gi_send.at[k, p], recv.at[p], where
        ).start()

    def own_part(k, p):
        target = (f, partner)[k]
        value = input_part(k, p)

        @pl.when(hub)
        def _():
            hub_f32[k, half_rows(p), :] = value

        @pl.when(jnp.logical_not(hub))
        def _():
            gi_out[k, half_rows(p), :] = value.astype(BF16)

        if k == 0:
            @pl.when(home)
            def _():
                gi_in[0, half_rows(p), :] = gi_out[k, half_rows(p), :]
        else:
            @pl.when(home)
            def _():
                input_send(k, p, gi_in.at[0], gi_recv.at[0], {"fs": target})

        @pl.when(near)
        def _():
            input_send(k, p, gi_in.at[2], gi_recv.at[2], {"fs": target, "tp": f})

        @pl.when(jnp.logical_not(home | near | hub))
        def _():
            input_send(k, p, near_in.at[k], near_recv.at[k], {"tp": z_pair})

    def own_sum(k, p):
        target = (f, partner)[k]

        @pl.when(hub)
        def _():
            input_sum(k, p, hub_f32[k, half_rows(p), :])
            input_send(k, p, gi_in.at[1], gi_recv.at[1], {"fs": target, "tp": f})

    def cross_part(k, p):
        value = input_part(k, p)

        @pl.when(direct)
        def _():
            hub_f32[k, half_rows(p), :] = value

        @pl.when(jnp.logical_not(direct))
        def _():
            gi_out[k, half_rows(p), :] = value.astype(BF16)
            input_send(k, p, near_in.at[k], near_recv.at[k], {"tp": z_pair})

    def cross_sum(k, p):
        target = (across, corner)[k - 2]

        @pl.when(direct)
        def _():
            input_sum(k, p, hub_f32[k, half_rows(p), :])

        @pl.when(home)
        def _():
            input_send(k, p, gi_in.at[0], gi_recv.at[0], {"fs": target})

        @pl.when(hub)
        def _():
            input_send(k, p, gi_mid, mid_recv, {"fs": target})

    for p in range(pieces):
        own_part(0, p)
    for p in range(pieces):
        for e in range(parts):
            dpre_landed(partner, e, p)
        own_part(1, p)

    def up_step(e, q):
        value = dot(
            acts_cols[:, q * gu_rows:(q + 1) * gu_rows], dpre_group[:, e * hp:(e + 1) * hp],
            ((0,), (0,)),
        )
        gu_out[e, q] = (value * norm_factor).astype(BF16)
        for p in range(1, reps):
            rep_copy(gu_out, gu_in, gu_send, gu_recv, (e, q), p).start()

    for e in range(parts):
        last = e == parts - 1
        for p in range(pieces):
            dpre_step(1, across, e, p)
            dpre_landed(corner, e, p)
            if last:
                cross_part(2, p)
                cross_part(3, p)
        if e == 0:
            for p in range(strips):
                @pl.when(jnp.logical_not(direct))
                def _():
                    cross_rest(1, p)

                line_landed(1, p)
        for q in range(tiles):
            up_step(e, q)
    for p in range(pieces):
        for k in range(2):
            own_sum(k, p)
    for p in range(pieces):
        for k in range(2, 4):
            cross_sum(k, p)

    relays = lax.div(z_far, 2) != place
    for p in range(pieces):
        @pl.when(relays)
        def _():
            ref = gi_mid.at[half_rows(p)]
            landed(ref, mid_recv.at[p])
            remote(
                ref, gi_in.at[1, half_rows(p)], relay_send.at[p], gi_recv.at[1, p], {"tp": z_far}
            ).start()

    for p in range(1, reps):
        for c in range(steps):
            rep_copy(gd_out, gd_in, gd_send, gd_recv, (c,), p).wait()
    for p in range(pieces):
        @pl.when(jnp.logical_not(home))
        def _():
            landed(gi_in.at[0, half_rows(p)], gi_recv.at[0, p])

        landed(gi_in.at[1, half_rows(p)], gi_recv.at[1, p])

        @pl.when(same)
        def _():
            landed(gi_in.at[2, half_rows(p)], gi_recv.at[2, p])

    for p in range(strips):
        for a in range(2):
            @pl.when(same & (z != f) | jnp.logical_not(same))
            def _():
                left_for(own.at[pl.ds(p * sp, sp)], org_send.at[a, 0, p])

            @pl.when(direct)
            def _():
                for source in (across, corner):
                    left_for(own.at[pl.ds(p * sp, sp)], fwd_send.at[a, source, p])

        @pl.when(jnp.logical_not(same))
        def _():
            for a in range(2):
                left_for(own.at[pl.ds(p * sp, sp)], org_send.at[a, 1, p])

        @pl.when(same & (z < T - 1))
        def _():
            left_for(own.at[pl.ds(p * sp, sp)], org_send.at[0, 1, p])

        @pl.when(same & (z > 0))
        def _():
            left_for(own.at[pl.ds(p * sp, sp)], org_send.at[0, 2, p])

        @pl.when(rises | falls)
        def _():
            for source in (f, partner):
                left_for(own.at[pl.ds(p * sp, sp)], fwd_send.at[0, source, p])

        for k in range(1, T - 1):
            @pl.when(same & ((z + k < T - 1) | ((k == 1) & (z + k < T))))
            def _():
                left_for(own.at[pl.ds(p * sp, sp)], org_send.at[1, T + k, p])

            @pl.when(same & ((z - k > 0) | ((k == 1) & (z - k >= 0))))
            def _():
                left_for(own.at[pl.ds(p * sp, sp)], org_send.at[1, 1 + k, p])

        @pl.when(last_up | last_down)
        def _():
            for source in (f, partner):
                left_for(own.at[pl.ds(p * sp, sp)], fwd_send.at[1, source, p])

    for p in range(pieces):
        @pl.when(jnp.logical_not(home))
        def _():
            left_for(own.at[half_rows(p)], gi_send.at[0, p])

        for k in range(1, 4):
            left_for(own.at[half_rows(p)], gi_send.at[k, p])

        @pl.when(relays)
        def _():
            left_for(own.at[half_rows(p)], relay_send.at[p])

        for k in range(2):
            left_for(pair_out.at[k, p], pair_send.at[k, p])
            for e in range(parts):
                left_for(dpre_group.at[piece(f, p), hidden(e)], dpre_send.at[k, e, p])
                left_for(far_out.at[k, e, p], far_send.at[k, e, p])
    for k in range(3):
        for c in range(steps):
            left_for(pos_group.at[rows(f), act_cols(c)], act_send.at[k, c])
    for p in range(1, reps):
        for e in range(parts):
            for q in range(tiles):
                rep_copy(gu_out, gu_in, gu_send, gu_recv, (e, q), p).wait()


def finish_kernel(
    gd_out, gd_in, gu_out, gu_in, gi_in, grad_input, grad_up, grad_down,
    gi_v, gu_v, gd_v, gi_sem, gu_sem, gd_sem,
):
    others = gd_in.shape[0]
    steps, gd_rows = gd_out.shape[0], gd_out.shape[1]
    parts, tiles, gu_rows, hp = gu_out.shape
    copies = []

    def leave(src, dst, sem):
        copies.append(pltpu.make_async_copy(src, dst, sem))
        copies[-1].start()

    for c in range(steps):
        value = gd_out[c].astype(F32)
        for p in range(others):
            value = value + gd_in[p, c].astype(F32)
        gd_v[c] = value
        leave(gd_v.at[c], grad_down.at[pl.ds(c * gd_rows, gd_rows)], gd_sem.at[c])
    for e in range(parts):
        for q in range(tiles):
            value = gu_out[e, q].astype(F32)
            for p in range(others):
                value = value + gu_in[p, e, q].astype(F32)
            gu_v[e, q] = value
            at = (pl.ds(q * gu_rows, gu_rows), pl.ds(e * hp, hp))
            leave(gu_v.at[e, q], grad_up.at[at], gu_sem.at[e, q])
    value = gi_in[0].astype(F32)
    for s in range(1, gi_in.shape[0]):
        value = value + gi_in[s].astype(F32)
    gi_v[...] = value.astype(BF16)
    leave(gi_v, grad_input, gi_sem.at[0])
    for copy in copies:
        copy.wait()


def square_body(sizes, acts, cotangent, pre_act, up_store, up_scale, down_store, down_scale):
    reps, F, T = sizes
    n, d = acts.shape
    h = pre_act.shape[1]
    w = down_store.shape[1]
    parts = 2 if h % 256 == 0 else 1
    pieces = 2 if n % 32 == 0 else 1
    tiles = 2 if w % 256 == 0 else 1
    strips = 2 * pieces if n % 64 == 0 else pieces
    hp, rp = h // parts, n // pieces
    gd_rows = fitting(h, 256)
    steps = h // gd_rows
    others = reps - 1
    sem = pltpu.SemaphoreType.DMA
    vmem, hbm = (pl.BlockSpec(memory_space=s) for s in (pltpu.VMEM, pltpu.HBM))
    shared = [
        (steps, gd_rows, w), (others, steps, gd_rows, w),
        (parts, tiles, w // tiles, hp), (others, parts, tiles, w // tiles, hp),
        (3, n, w),
    ]
    arrays = [
        ((n, d), BF16), ((n, d), BF16), ((n, h), BF16),
        ((w, h), F32), ((1, h), F32), ((h, w), F32), ((1, d * T), F32),
        ((n, d), BF16), ((F * n, w), BF16), ((F * n, w), BF16),
        ((F * n, h), BF16), ((F * n, h), BF16),
        ((h, w), BF16), ((w, h), BF16),
        ((2, pieces, rp, h), BF16), ((2, pieces, rp, h), BF16),
        ((2, parts, pieces, rp, hp), BF16), ((2, parts, pieces, rp, hp), BF16),
        ((2, pieces, rp, h), F32),
        ((F, n, w), BF16), ((n, w), BF16), ((F, n, w), BF16), ((F, n, w), F32),
    ]
    moved = pl.pallas_call(
        functools.partial(square_kernel, sizes),
        out_shape=tuple(jax.ShapeDtypeStruct(shape, BF16) for shape in shared),
        in_specs=[hbm] * 7,
        out_specs=(vmem,) * len(shared),
        scratch_shapes=[pltpu.VMEM(shape, kind) for shape, kind in arrays] + [
            sem((7,)),
            sem((2, 2 * T, strips)), sem((2, F, strips)), sem((2, F, strips)),
            sem((3, steps)), sem((F, steps)), sem((2, parts, pieces)), sem((parts, F, pieces)),
            sem((2, pieces)), sem((2, pieces)), sem((2, parts, pieces)), sem((2, parts, pieces)),
            sem((pieces,)), sem((F, pieces)), sem((F, pieces)), sem((3, pieces)), sem((pieces,)),
            sem((others, steps)), sem((others, steps)),
            sem((others, parts, tiles)), sem((others, parts, tiles)),
        ],
        compiler_params=pltpu.CompilerParams(
            collective_id=0, has_side_effects=True,
            vmem_limit_bytes=40 * 1024 * 1024,
        ),
    )(*(
        pltpu.with_memory_space_constraint(array, pltpu.HBM)
        for array in (
            acts, cotangent, pre_act, up_store, up_scale.reshape(1, h), down_store,
            down_scale.reshape(1, d * T),
        )
    ))
    return pl.pallas_call(
        finish_kernel,
        out_shape=(
            jax.ShapeDtypeStruct((n, d), BF16),
            jax.ShapeDtypeStruct((w, h), F32),
            jax.ShapeDtypeStruct((h, w), F32),
        ),
        in_specs=[vmem] * len(shared),
        out_specs=(hbm,) * 3,
        scratch_shapes=[
            pltpu.VMEM((n, d), BF16),
            pltpu.VMEM((parts, tiles, w // tiles, hp), F32),
            pltpu.VMEM((steps, gd_rows, w), F32),
            sem((1,)), sem((parts, tiles)), sem((steps,)),
        ],
        compiler_params=pltpu.CompilerParams(vmem_limit_bytes=12 * 1024 * 1024),
    )(*moved)


def body(sizes, *arrays):
    reps, F, T = sizes
    square = F == T and F == 2 * 2 and reps > 1
    return (square_body if square else general_body)(sizes, *arrays)


def solution(mesh):
    sizes = (mesh.shape["rep"], mesh.shape["fs"], mesh.shape["tp"])
    return jax.shard_map(
        functools.partial(body, sizes),
        mesh=mesh,
        in_specs=(
            P(("rep", "fs"), "tp"),
            P(("rep", "fs"), "tp"),
            P(("rep", "fs"), "tp"),
            P("fs", "tp"),
            P("tp"),
            P("tp", "fs"),
            P(),
        ),
        out_specs=(P(("rep", "fs"), "tp"), P("fs", "tp"), P("tp", "fs")),
        check_vma=False,
    )
```

```python
import functools
import math

import jax
import jax.numpy as jnp
from jax import lax
from jax.experimental import pallas as pl
from jax.experimental.pallas import tpu as pltpu
from jax.sharding import PartitionSpec as P

F32, BF16 = jnp.float32, jnp.bfloat16


def dot(left, right, dims):
    return lax.dot_general(left, right, (dims, ((), ())), preferred_element_type=F32)


def fitting(size, most):
    return most if size % most == 0 else size


def general_kernel(
    sizes,
    acts, cotangent, pre_act, up_store, up_scale, down_store, down_scale,
    grad_input, grad_up, grad_down,
    up_f32, down_f32,
    blocks, scaled_cols, acts_cols, act_group, dpre_group, down_bf, up_bf,
    pair_out, pair_in, far_out, far_in, d_act, gi_out, gi_mid, gi_in,
    gd_out, gd_in, gu_out, gu_in,
    load_sem,
    z_send, z_recv, col_send, col_recv, act_send, act_recv, dpre_send, dpre_recv,
    pair_send, pair_recv, far_send, far_recv, mid_send, mid_recv, gi_send, gi_recv,
    gd_send, gd_recv, gu_send, gu_recv,
):
    reps, F, T = sizes
    n, d = acts.shape
    h = pre_act.shape[1]
    w = down_store.shape[1]
    half, sub = F // 2, F // T
    chunks, cw = blocks.shape[2], blocks.shape[4]
    per = w // cw
    parts, hp = dpre_group.shape[0], dpre_group.shape[2]
    norm_factor = 1.0 / math.sqrt(n * F * reps)
    r, f, z = lax.axis_index("rep"), lax.axis_index("fs"), lax.axis_index("tp")
    core, place = lax.rem(f, 2), lax.div(f, 2)
    partner = f + 1 - 2 * core
    mesh_ids = pl.DeviceIdType.MESH

    down_load = pltpu.make_async_copy(down_store, down_f32, load_sem.at[0])
    up_load = pltpu.make_async_copy(up_store, up_f32, load_sem.at[1])
    down_load.start()
    up_load.start()

    barrier = pltpu.get_barrier_semaphore()

    def greet(at, carry):
        to_f, to_z = lax.div(at, T), lax.rem(at, T)

        @pl.when((to_f != f) | (to_z != z))
        def _():
            pl.semaphore_signal(
                barrier, inc=1, device_id={"fs": to_f, "tp": to_z}, device_id_type=mesh_ids
            )

        return carry

    lax.fori_loop(0, F * T, greet, 0)
    for p in range(1, reps):
        pl.semaphore_signal(
            barrier, inc=1, device_id={"rep": lax.rem(r + p, reps)}, device_id_type=mesh_ids
        )

    def rows(at):
        return pl.ds(pl.multiple_of(at * n, n), n)

    def remote(src, dst, send, recv, where):
        return pltpu.make_async_remote_copy(
            src_ref=src, dst_ref=dst, send_sem=send, recv_sem=recv,
            device_id=where, device_id_type=mesh_ids,
        )

    def landed(ref, recv):
        remote(ref, ref, recv, recv, {"fs": partner}).wait_recv()

    def left_for(ref, send):
        remote(ref, ref, send, send, {"fs": partner}).wait_send()

    cols = (scaled_cols, acts_cols)

    def pass_on(a, block, g, way):
        @pl.when((z < T - 1) if way == 0 else (z > 0))
        def _():
            ref = blocks.at[a, block, g]
            to = z + 1 if way == 0 else z - 1
            remote(ref, ref, z_send.at[a, block, g, way], z_recv.at[a, block, g], {"tp": to}).start()

    def spread(a, block, g):
        target, q = block * sub + g // per, g % per

        @pl.when(target != f)
        def _():
            remote(
                blocks.at[a, block, g], cols[a].at[q, rows(f)],
                col_send.at[a, block, g], col_recv.at[a, f, q], {"fs": target},
            ).start()

        @pl.when(target == f)
        def _():
            cols[a][q, rows(f), :] = blocks[a, block, g]

    def own_block(a):
        for g in range(chunks):
            pass_on(a, z, g, 0)
            pass_on(a, z, g, 1)
        for g in range(chunks):
            spread(a, z, g)

    def arriving(a, s):
        for g in range(chunks):
            @pl.when(z - s >= 0)
            def _():
                landed(blocks.at[a, z - s, g], z_recv.at[a, z - s, g])
                pass_on(a, z - s, g, 0)
                spread(a, z - s, g)

            @pl.when(z + s <= T - 1)
            def _():
                landed(blocks.at[a, z + s, g], z_recv.at[a, z + s, g])
                pass_on(a, z + s, g, 1)
                spread(a, z + s, g)

    def cols_landed(a, source):
        @pl.when(source != f)
        def _():
            for q in range(per):
                landed(cols[a].at[q, rows(source)], col_recv.at[a, source, q])

    def group_start(group, send, recv):
        ref = group.at[rows(f)]
        for k in range(1, half):
            to = lax.rem(f + 2 * k, F)
            remote(ref, ref, send.at[k], recv.at[f], {"fs": to}).start()
        remote(ref, ref, send.at[0], recv.at[f], {"fs": partner}).start()

    def group_forward(group, send, recv):
        for k in range(1, half):
            source = lax.rem(f - 2 * k + F, F)
            ref = group.at[rows(source)]
            landed(ref, recv.at[source])
            remote(ref, ref, send.at[half - 1 + k], recv.at[source], {"fs": partner}).start()

    def forwards_landed(group, recv):
        for k in range(1, half):
            source = lax.rem(partner + 2 * k, F)
            landed(group.at[rows(source)], recv.at[source])

    def group_sent(group, send):
        for k in range(F - 1):
            left_for(group.at[rows(f)], send.at[k])

    scale = down_scale[:, pl.ds(pl.multiple_of(z * d, d), d)]
    scaled = (cotangent[...].astype(F32) * scale).astype(BF16)
    for g in range(chunks):
        blocks[0, z, g] = scaled[:, g * cw:(g + 1) * cw]
    positive = jnp.maximum(pre_act[...].astype(F32), 0.0)
    act_group[rows(f), :] = (positive * positive).astype(BF16)
    pl.semaphore_wait(barrier, F * T - 1 + reps - 1)
    own_block(0)
    group_start(act_group, act_send, act_recv)
    for g in range(chunks):
        blocks[1, z, g] = acts[:, g * cw:(g + 1) * cw]
    down_load.wait()
    down_bf[...] = down_f32[...].astype(BF16)
    for s in range(1, T):
        if s == T - 1:
            group_forward(act_group, act_send, act_recv)
        arriving(0, s)
    own_block(1)

    def partial_of(target, e):
        value = jnp.zeros((n, hp), F32)
        for q in range(per):
            value = value + dot(
                scaled_cols[q, rows(target), :],
                down_bf[e * hp:(e + 1) * hp, q * cw:(q + 1) * cw], ((1,), (1,)),
            )
        return value

    for e in range(parts):
        def for_partner(k, carry):
            i = lax.rem(place + k, half)
            if e == 0:
                cols_landed(0, 2 * i + 1 - core)
            pair_out[e, i] = partial_of(2 * i + 1 - core, e).astype(BF16)
            remote(
                pair_out.at[e, i], pair_in.at[e, i], pair_send.at[e, i], pair_recv.at[e, i],
                {"fs": partner},
            ).start()
            return carry

        lax.fori_loop(1, half + 1, for_partner, 0)
    for e in range(parts):
        def for_far(k, carry):
            i = lax.rem(place + k, half)
            if e == 0:
                cols_landed(0, 2 * i + core)
            value = partial_of(2 * i + core, e)
            landed(pair_in.at[e, i], pair_recv.at[e, i])
            far_out[e, i] = (value + pair_in[e, i].astype(F32)).astype(BF16)
            remote(
                far_out.at[e, i], far_in.at[e, place], far_send.at[e, i], far_recv.at[e, place],
                {"fs": 2 * i + core},
            ).start()
            return carry

        lax.fori_loop(1, half, for_far, 0)
    for e in range(parts):
        value = partial_of(f, e)
        landed(pair_in.at[e, place], pair_recv.at[e, place])
        d_act[e] = value + pair_in[e, place].astype(F32)

    landed(act_group.at[rows(partner)], act_recv.at[partner])
    forwards_landed(act_group, act_recv)
    gd_rows = gd_out.shape[1]

    def rep_copy(out, into, send, recv, c, p):
        to = lax.rem(r + p, reps)
        return remote(
            out.at[c], into.at[p - 1, c], send.at[p - 1, c], recv.at[p - 1, c], {"rep": to}
        )

    def down_step(c, carry):
        at = pl.ds(pl.multiple_of(c * gd_rows, gd_rows), gd_rows)
        for q in range(per):
            value = dot(act_group[:, at], scaled_cols[q], ((0,), (0,))) * norm_factor
            gd_out[c, :, q * cw:(q + 1) * cw] = value.astype(BF16)
        for p in range(1, reps):
            rep_copy(gd_out, gd_in, gd_send, gd_recv, c, p).start()
        return carry

    lax.fori_loop(0, gd_out.shape[0], down_step, 0)
    arriving(1, 1)
    for e in range(parts):
        total = d_act[e]
        for k in range(1, half):
            j = lax.rem(place + k, half)
            landed(far_in.at[e, j], far_recv.at[e, j])
            total = total + far_in[e, j].astype(F32)
        at = slice(e * hp, (e + 1) * hp)
        positive = jnp.maximum(pre_act[:, at].astype(F32), 0.0)
        dpre_group[e, rows(f), :] = (2.0 * positive * total * up_scale[:, at]).astype(BF16)
        group_start(dpre_group.at[e], dpre_send.at[e], dpre_recv.at[e])
        if e == 0:
            up_load.wait()
            up_bf[...] = up_f32[...].astype(BF16)
            for s in range(2, T - 1):
                arriving(1, s)
    if T > 2:
        arriving(1, T - 1)

    def send_home(ref, source):
        home, slot = lax.div(source, sub), z * sub + lax.rem(source, sub)

        @pl.when(home != z)
        def _():
            remote(
                ref, gi_in.at[slot], gi_send.at[source], gi_recv.at[slot], {"tp": home}
            ).start()

        @pl.when(home == z)
        def _():
            gi_in[slot] = ref[...]

    def input_part(source):
        value = jnp.zeros((n, w), F32)
        for e in range(parts):
            value = value + dot(
                dpre_group[e, rows(source), :], up_bf[:, e * hp:(e + 1) * hp], ((1,), (1,))
            )
        gi_out[source] = value.astype(BF16)

        if source is f:
            send_home(gi_out.at[source], f)
        else:
            remote(
                gi_out.at[source], gi_mid.at[f], mid_send.at[source], mid_recv.at[f],
                {"fs": source},
            ).start()

    def relay(source):
        landed(gi_mid.at[source], mid_recv.at[source])
        send_home(gi_mid.at[source], source)

    input_part(f)
    for e in range(parts):
        landed(dpre_group.at[e, rows(partner)], dpre_recv.at[e, partner])
    input_part(partner)
    relay(partner)

    def up_step(e):
        forwards_landed(dpre_group.at[e], dpre_recv.at[e])
        for q in range(per):
            value = dot(acts_cols[q], dpre_group[e], ((0,), (0,)))
            gu_out[e, q * cw:(q + 1) * cw, :] = (value * norm_factor).astype(BF16)
        for p in range(1, reps):
            rep_copy(gu_out, gu_in, gu_send, gu_recv, e, p).start()

    for e in range(parts):
        group_forward(dpre_group.at[e], dpre_send.at[e], dpre_recv.at[e])
        if e == 0:
            for source in range(F):
                cols_landed(1, source)
        if e < parts - 1:
            up_step(e)
    for k in range(1, half):
        input_part(lax.rem(f + 2 * k, F))
    forwards_landed(dpre_group.at[parts - 1], dpre_recv.at[parts - 1])
    for k in range(1, half):
        input_part(lax.rem(partner + 2 * k, F))
    for q in range(per):
        value = dot(acts_cols[q], dpre_group[parts - 1], ((0,), (0,)))
        gu_out[parts - 1, q * cw:(q + 1) * cw, :] = (value * norm_factor).astype(BF16)
    for p in range(1, reps):
        rep_copy(gu_out, gu_in, gu_send, gu_recv, parts - 1, p).start()
    for k in range(1, half):
        relay(lax.rem(f + 2 * k, F))
        relay(lax.rem(partner + 2 * k, F))

    def total_of(out, into, send, recv, c):
        for p in range(1, reps):
            rep_copy(out, into, send, recv, c, p).wait()
        value = out[c].astype(F32)
        for p in range(1, reps):
            value = value + into[p - 1, c].astype(F32)
        return value

    def finish_down(c, carry):
        at = pl.ds(pl.multiple_of(c * gd_rows, gd_rows), gd_rows)
        grad_down[at, :] = total_of(gd_out, gd_in, gd_send, gd_recv, c)
        return carry

    lax.fori_loop(0, gd_out.shape[0], finish_down, 0)
    for e in range(parts - 1):
        grad_up[:, e * hp:(e + 1) * hp] = total_of(gu_out, gu_in, gu_send, gu_recv, e)
    for j in range(sub):
        value = jnp.zeros((n, w), F32)
        for s in range(T):
            at = s * sub + j

            @pl.when(s != z)
            def _():
                landed(gi_in.at[at], gi_recv.at[at])

            value = value + gi_in[at].astype(F32)
        grad_input[:, j * w:(j + 1) * w] = value.astype(BF16)
    grad_up[:, (parts - 1) * hp:] = total_of(gu_out, gu_in, gu_send, gu_recv, parts - 1)

    for a in range(2):
        for block in range(T):
            for g in range(chunks):
                @pl.when((block <= z) & (z < T - 1))
                def _():
                    left_for(blocks.at[a, block, g], z_send.at[a, block, g, 0])

                @pl.when((block >= z) & (z > 0))
                def _():
                    left_for(blocks.at[a, block, g], z_send.at[a, block, g, 1])

                @pl.when(block * sub + g // per != f)
                def _():
                    left_for(blocks.at[a, block, g], col_send.at[a, block, g])
    group_sent(act_group, act_send)
    for e in range(parts):
        group_sent(dpre_group.at[e], dpre_send.at[e])
        for i in range(half):
            left_for(pair_out.at[e, i], pair_send.at[e, i])

            @pl.when(i != place)
            def _():
                left_for(far_out.at[e, i], far_send.at[e, i])
    for source in range(F):
        @pl.when(source != f)
        def _():
            left_for(gi_out.at[source], mid_send.at[source])

        @pl.when(source // sub != z)
        def _():
            left_for(gi_mid.at[source], gi_send.at[source])


def general_body(sizes, acts, cotangent, pre_act, up_store, up_scale, down_store, down_scale):
    reps, F, T = sizes
    n, d = acts.shape
    h = pre_act.shape[1]
    w = down_store.shape[1]
    half = F // 2
    cw = w // 2 if w % 256 == 0 else w
    per, chunks = w // cw, d // cw
    parts = 2 if h % 256 == 0 else 1
    hp = h // parts
    gd_rows = fitting(h, 256)
    gd_steps = h // gd_rows
    others = max(reps - 1, 1)
    sem = pltpu.SemaphoreType.DMA
    vmem, anywhere = (pl.BlockSpec(memory_space=s) for s in (pltpu.VMEM, pltpu.HBM))
    arrays = [
        ((w, h), F32), ((h, w), F32),
        ((2, T, chunks, n, cw), BF16),
        ((per, F * n, cw), BF16), ((per, F * n, cw), BF16),
        ((F * n, h), BF16), ((parts, F * n, hp), BF16),
        ((h, w), BF16), ((w, h), BF16),
        ((parts, half, n, hp), BF16), ((parts, half, n, hp), BF16),
        ((parts, half, n, hp), BF16), ((parts, half, n, hp), BF16),
        ((parts, n, hp), F32),
        ((F, n, w), BF16), ((F, n, w), BF16), ((F, n, w), BF16),
        ((gd_steps, gd_rows, w), BF16), ((others, gd_steps, gd_rows, w), BF16),
        ((parts, w, hp), BF16), ((others, parts, w, hp), BF16),
    ]
    return pl.pallas_call(
        functools.partial(general_kernel, sizes),
        out_shape=(
            jax.ShapeDtypeStruct((n, d), BF16),
            jax.ShapeDtypeStruct((w, h), F32),
            jax.ShapeDtypeStruct((h, w), F32),
        ),
        in_specs=[vmem, vmem, vmem, anywhere, vmem, anywhere, vmem],
        out_specs=(vmem, vmem, vmem),
        scratch_shapes=[pltpu.VMEM(shape, kind) for shape, kind in arrays] + [
            sem((2,)),
            sem((2, T, chunks, 2)), sem((2, T, chunks)), sem((2, T, chunks)), sem((2, F, per)),
            sem((F,)), sem((F,)), sem((parts, F)), sem((parts, F)),
            sem((parts, half)), sem((parts, half)), sem((parts, half)), sem((parts, half)),
            sem((F,)), sem((F,)), sem((F,)), sem((F,)),
            sem((others, gd_steps)), sem((others, gd_steps)),
            sem((others, parts)), sem((others, parts)),
        ],
        compiler_params=pltpu.CompilerParams(
            collective_id=0, has_side_effects=True,
            vmem_limit_bytes=60 * 1024 * 1024,
        ),
    )(
        acts, cotangent, pre_act, up_store, up_scale.reshape(1, h), down_store,
        down_scale.reshape(1, d * T),
    )


def square_kernel(
    sizes,
    acts, cotangent, pre_act, up_store, up_scale, down_store, down_scale,
    gd_out, gd_in, gu_out, gu_in, gi_in,
    acts_v, cot_v, pre_v, up_f32, up_scale_v, down_f32, down_scale_v,
    own, scaled_cols, acts_cols, pos_group, dpre_group, down_bf, up_bf,
    pair_out, pair_in, far_out, far_in, sums, gi_out, gi_mid, near_in, hub_f32,
    load_sem,
    org_send, fwd_send, col_recv, act_send, act_recv, dpre_send, dpre_recv,
    pair_send, pair_recv, far_send, far_recv,
    mid_recv, near_recv, gi_send, gi_recv, relay_send,
    gd_send, gd_recv, gu_send, gu_recv,
):
    reps, F, T = sizes
    n, d = acts.shape
    h = pre_act.shape[1]
    w = down_store.shape[1]
    steps, gd_rows = gd_out.shape[0], gd_out.shape[1]
    parts, tiles, gu_rows, hp = gu_out.shape
    pieces, strips = sums.shape[1], col_recv.shape[2]
    rp, sp = n // pieces, n // strips
    norm_factor = 1.0 / math.sqrt(n * F * reps)
    r, f, z = lax.axis_index("rep"), lax.axis_index("fs"), lax.axis_index("tp")
    core, place = lax.rem(f, 2), lax.div(f, 2)
    partner = f + 1 - 2 * core
    across = lax.rem(f + 2, F)
    corner = lax.rem(partner + 2, F)
    z_pair, z_far = z + 1 - 2 * lax.rem(z, 2), lax.rem(z + 2, T)
    mesh_ids = pl.DeviceIdType.MESH

    loads = [
        pltpu.make_async_copy(src, dst, load_sem.at[i])
        for i, (src, dst) in enumerate((
            (cotangent, cot_v), (down_scale, down_scale_v), (pre_act, pre_v),
            (down_store, down_f32), (acts, acts_v), (up_scale, up_scale_v), (up_store, up_f32),
        ))
    ]
    for load in loads:
        load.start()

    barrier = pltpu.get_barrier_semaphore()

    def greet(at, carry):
        to_f, to_z = lax.div(at, T), lax.rem(at, T)

        @pl.when((to_f != f) | (to_z != z))
        def _():
            pl.semaphore_signal(
                barrier, inc=1, device_id={"fs": to_f, "tp": to_z}, device_id_type=mesh_ids
            )

        return carry

    lax.fori_loop(0, F * T, greet, 0)
    for p in range(1, reps):
        pl.semaphore_signal(
            barrier, inc=1, device_id={"rep": lax.rem(r + p, reps)}, device_id_type=mesh_ids
        )

    def rows(at):
        return pl.ds(pl.multiple_of(at * n, n), n)

    def piece(at, p):
        return pl.ds(pl.multiple_of(at * n + p * rp, rp), rp)

    def strip(at, p):
        return pl.ds(pl.multiple_of(at * n + p * sp, sp), sp)

    def strips_of(p):
        return range(p * strips // pieces, (p + 1) * strips // pieces)

    def remote(src, dst, send, recv, where):
        return pltpu.make_async_remote_copy(
            src_ref=src, dst_ref=dst, send_sem=send, recv_sem=recv,
            device_id=where, device_id_type=mesh_ids,
        )

    def landed(ref, recv):
        remote(ref, ref, recv, recv, {"fs": partner}).wait_recv()

    def left_for(ref, send):
        remote(ref, ref, send, send, {"fs": partner}).wait_send()

    cols = (scaled_cols, acts_cols)
    sources = (own, acts_v)
    same = lax.div(z, 2) == place
    direct = (z == f) | (z_far == f)
    home, hub, near = z == f, z_far == f, z_pair == f
    rises = (z > f) & (z < T - 1)
    falls = (z < f) & (z > 0)

    def originate(a, k, p, where):
        at = pl.ds(p * sp, sp)
        remote(
            sources[a].at[at], cols[a].at[strip(f, p)],
            org_send.at[a, k, p], col_recv.at[a, f, p], where,
        ).start()

    def originate_line(a):
        @pl.when(same)
        def _():
            for p in range(strips):
                @pl.when(z < T - 1)
                def _():
                    originate(a, 1, p, {"fs": z, "tp": z + 1})

                @pl.when(z > 0)
                def _():
                    originate(a, 2, p, {"fs": z, "tp": z - 1})

                @pl.when(z != f)
                def _():
                    originate(a, 0, p, {"fs": z})

            @pl.when(z == f)
            def _():
                cols[a][rows(f), :] = sources[a][...]

    def spread_inner(a):
        @pl.when(same)
        def _():
            for p in range(strips):
                for k in range(1, T - 1):
                    @pl.when(z + k < T - 1)
                    def _():
                        originate(a, T + k, p, {"fs": z, "tp": z + k})

                    @pl.when(z - k > 0)
                    def _():
                        originate(a, 1 + k, p, {"fs": z, "tp": z - k})

    def spread_outer(a):
        @pl.when(same)
        def _():
            for p in range(strips):
                @pl.when(z == T - 2)
                def _():
                    originate(a, T + 1, p, {"fs": z, "tp": z + 1})

                @pl.when(z == 1)
                def _():
                    originate(a, 2, p, {"fs": z, "tp": z - 1})

                @pl.when(z != f)
                def _():
                    originate(a, 0, p, {"fs": z})

            @pl.when(z == f)
            def _():
                cols[a][rows(f), :] = sources[a][...]

    def originate_cross(a):
        @pl.when(jnp.logical_not(same))
        def _():
            for p in range(strips):
                originate(a, 1, p, {"fs": z, "tp": z_far})
                if a == 0:
                    originate(a, 0, p, {"fs": z})

    def pass_on(a, source, p, to):
        ref = cols[a].at[strip(source, p)]
        landed(ref, col_recv.at[a, source, p])
        remote(ref, ref, fwd_send.at[a, source, p], col_recv.at[a, source, p], {"tp": to}).start()

    def cross_forward(a, p):
        for source in (across, corner):
            pass_on(a, source, p, z_pair)

    def line_forward(a, p):
        @pl.when(rises)
        def _():
            for source in (f, partner):
                pass_on(a, source, p, z + 1)

        @pl.when(falls)
        def _():
            for source in (f, partner):
                pass_on(a, source, p, z - 1)

    def cross_rest(a, p):
        for source in (across, corner):
            landed(cols[a].at[strip(source, p)], col_recv.at[a, source, p])

    last_up, last_down = (z > f) & (z == T - 2), (z < f) & (z == 1)

    def tip_forward(a, p):
        @pl.when(last_up)
        def _():
            for source in (f, partner):
                pass_on(a, source, p, z + 1)

        @pl.when(last_down)
        def _():
            for source in (f, partner):
                pass_on(a, source, p, z - 1)

    def line_landed(a, p):
        @pl.when(jnp.logical_not(last_up | last_down) & (z != f))
        def _():
            landed(cols[a].at[strip(f, p)], col_recv.at[a, f, p])

        @pl.when(jnp.logical_not(last_up | last_down))
        def _():
            landed(cols[a].at[strip(partner, p)], col_recv.at[a, partner, p])

    def line_rest(a, p):
        @pl.when(jnp.logical_not(rises | falls) & (z != f))
        def _():
            landed(cols[a].at[strip(f, p)], col_recv.at[a, f, p])

        @pl.when(jnp.logical_not(rises | falls))
        def _():
            landed(cols[a].at[strip(partner, p)], col_recv.at[a, partner, p])

    def act_cols(c):
        return pl.ds(pl.multiple_of(c * gd_rows, gd_rows), gd_rows)

    def act_send_to(source, c, k, where):
        ref = pos_group.at[rows(source), act_cols(c)]
        remote(ref, ref, act_send.at[k, c], act_recv.at[source, c], where).start()

    def act_landed(source, c):
        landed(pos_group.at[rows(source), act_cols(c)], act_recv.at[source, c])

    def act_forward(c):
        act_landed(across, c)
        act_send_to(across, c, 2, {"fs": partner})

    loads[0].wait()
    loads[1].wait()
    scale = down_scale_v[:, pl.ds(pl.multiple_of(z * d, d), d)]
    own[...] = (cot_v[...].astype(F32) * scale).astype(BF16)
    pl.semaphore_wait(barrier, F * T - 1 + reps - 1)
    originate_cross(0)
    originate_line(0)
    loads[2].wait()
    pos_group[rows(f), :] = jnp.maximum(pre_v[...].astype(F32), 0.0).astype(BF16)
    for c in range(steps):
        act_send_to(f, c, 0, {"fs": across})

    loads[4].wait()

    @pl.when(jnp.logical_not(same))
    def _():
        for p in range(strips):
            originate(1, 0, p, {"fs": z})
        gi_in[2] = jnp.zeros((n, w), BF16)

    for c in range(steps):
        act_send_to(f, c, 1, {"fs": partner})
    loads[3].wait()
    down_bf[...] = down_f32[...].T.astype(BF16)

    def partial_of(target, p):
        return dot(scaled_cols[piece(target, p), :], down_bf[...], ((1,), (0,)))

    def to_partner(target, k, p):
        pair_out[k, p] = partial_of(target, p).astype(BF16)
        remote(
            pair_out.at[k, p], pair_in.at[k, p], pair_send.at[k, p], pair_recv.at[k, p],
            {"fs": partner},
        ).start()

    def chip_sum(target, k, p):
        value = partial_of(target, p)
        landed(pair_in.at[k, p], pair_recv.at[k, p])
        value = value + pair_in[k, p].astype(F32)
        sums[k, p] = value
        for e in range(parts):
            far_out[k, e, p] = value[:, e * hp:(e + 1) * hp].astype(BF16)

    def far_start(k, e, p):
        remote(
            far_out.at[k, e, p], far_in.at[k, e, p], far_send.at[k, e, p], far_recv.at[k, e, p],
            {"fs": across},
        ).start()

    for p in range(pieces):
        for t in strips_of(p):
            @pl.when(direct)
            def _():
                cross_forward(0, t)

            line_forward(0, t)

        @pl.when(direct)
        def _():
            to_partner(corner, 0, p)

    def rep_copy(out, into, send, recv, at, p):
        to = lax.rem(r + p, reps)
        return remote(
            out.at[at], into.at[(p - 1,) + at], send.at[(p - 1,) + at], recv.at[(p - 1,) + at],
            {"rep": to},
        )

    def down_step(c, carry):
        act_landed(partner, c)
        act_landed(corner, c)
        positive = pos_group[:, act_cols(c)].astype(F32)
        act = (positive * positive).astype(BF16)
        value = dot(act, scaled_cols[...], ((0,), (0,))) * norm_factor
        gd_out[c] = value.astype(BF16)
        for p in range(1, reps):
            rep_copy(gd_out, gd_in, gd_send, gd_recv, (c,), p).start()
        return carry

    def forward_and_down(c, carry):
        act_forward(c)
        return down_step(c, carry)

    spread_inner(1)

    @pl.when(direct)
    def _():
        for p in range(strips):
            line_rest(0, p)
        lax.fori_loop(0, steps, forward_and_down, 0)

    for p in range(pieces):
        @pl.when(jnp.logical_not(direct))
        def _():
            for c in range(p * steps // pieces, (p + 1) * steps // pieces):
                act_forward(c)
            for t in strips_of(p):
                cross_rest(0, t)
            to_partner(corner, 0, p)

        chip_sum(across, 0, p)
        for e in range(parts if p == 0 else 1):
            far_start(0, e, p)
    originate_cross(1)
    spread_outer(1)

    @pl.when(jnp.logical_not(direct))
    def _():
        for p in range(strips):
            line_rest(0, p)
        lax.fori_loop(0, steps, down_step, 0)


    for p in range(strips):
        tip_forward(1, p)

    @pl.when(home)
    def _():
        for p in range(strips):
            cross_forward(1, p)

    for p in range(pieces):
        to_partner(partner, 1, p)
    for p in range(pieces):
        chip_sum(f, 1, p)
    for p in range(pieces):
        far_start(1, 0, p)
    for e in range(1, parts):
        for p in range(1, pieces):
            far_start(0, e, p)
        for p in range(pieces):
            far_start(1, e, p)
    loads[5].wait()
    loads[6].wait()
    up_bf[...] = up_f32[...].T.astype(BF16)

    def hidden(e):
        return pl.ds(e * hp, hp)

    def dpre_step(k, source, e, p):
        landed(far_in.at[k, e, p], far_recv.at[k, e, p])
        at = hidden(e)
        value = sums[1 - k, p, :, at] + far_in[k, e, p].astype(F32)
        positive = pos_group[piece(source, p), at].astype(F32)
        ref = dpre_group.at[piece(source, p), at]
        ref[...] = (2.0 * positive * value * up_scale_v[:, at]).astype(BF16)
        remote(ref, ref, dpre_send.at[k, e, p], dpre_recv.at[e, source, p], {"fs": partner}).start()

    def dpre_landed(source, e, p):
        landed(dpre_group.at[piece(source, p), hidden(e)], dpre_recv.at[e, source, p])

    @pl.when(hub)
    def _():
        for p in range(strips):
            cross_forward(1, p)

    for p in range(pieces):
        for e in range(parts if p == 0 else 1):
            dpre_step(0, f, e, p)

    def half_rows(p):
        return pl.ds(p * rp, rp)

    def input_part(k, p):
        target = (f, partner, across, corner)[k]
        return dot(dpre_group[piece(target, p), :], up_bf[...], ((1,), (0,)))

    def input_sum(k, p, value):
        landed(near_in.at[k, half_rows(p)], near_recv.at[k, p])
        gi_out[k, half_rows(p), :] = (value + near_in[k, half_rows(p), :].astype(F32)).astype(BF16)

    def input_send(k, p, into, recv, where):
        remote(
            gi_out.at[k, half_rows(p)], into.at[half_rows(p)], gi_send.at[k, p], recv.at[p], where
        ).start()

    def own_part(k, p):
        target = (f, partner)[k]
        value = input_part(k, p)

        @pl.when(hub)
        def _():
            hub_f32[k, half_rows(p), :] = value

        @pl.when(jnp.logical_not(hub))
        def _():
            gi_out[k, half_rows(p), :] = value.astype(BF16)

        if k == 0:
            @pl.when(home)
            def _():
                gi_in[0, half_rows(p), :] = gi_out[k, half_rows(p), :]
        else:
            @pl.when(home)
            def _():
                input_send(k, p, gi_in.at[0], gi_recv.at[0], {"fs": target})

        @pl.when(near)
        def _():
            input_send(k, p, gi_in.at[2], gi_recv.at[2], {"fs": target, "tp": f})

        @pl.when(jnp.logical_not(home | near | hub))
        def _():
            input_send(k, p, near_in.at[k], near_recv.at[k], {"tp": z_pair})

    def own_sum(k, p):
        target = (f, partner)[k]

        @pl.when(hub)
        def _():
            input_sum(k, p, hub_f32[k, half_rows(p), :])
            input_send(k, p, gi_in.at[1], gi_recv.at[1], {"fs": target, "tp": f})

    def cross_part(k, p):
        value = input_part(k, p)

        @pl.when(direct)
        def _():
            hub_f32[k, half_rows(p), :] = value

        @pl.when(jnp.logical_not(direct))
        def _():
            gi_out[k, half_rows(p), :] = value.astype(BF16)
            input_send(k, p, near_in.at[k], near_recv.at[k], {"tp": z_pair})

    def cross_sum(k, p):
        target = (across, corner)[k - 2]

        @pl.when(direct)
        def _():
            input_sum(k, p, hub_f32[k, half_rows(p), :])

        @pl.when(home)
        def _():
            input_send(k, p, gi_in.at[0], gi_recv.at[0], {"fs": target})

        @pl.when(hub)
        def _():
            input_send(k, p, gi_mid, mid_recv, {"fs": target})

    def own_parts(p):
        own_part(0, p)
        for e in range(parts) if p == 0 else range(parts - 1, parts):
            dpre_landed(partner, e, p)
        own_part(1, p)

    own_parts(0)

    def up_step(e, q):
        value = dot(
            acts_cols[:, q * gu_rows:(q + 1) * gu_rows], dpre_group[:, e * hp:(e + 1) * hp],
            ((0,), (0,)),
        )
        gu_out[e, q] = (value * norm_factor).astype(BF16)
        for p in range(1, reps):
            rep_copy(gu_out, gu_in, gu_send, gu_recv, (e, q), p).start()

    for e in range(parts):
        last = e == parts - 1
        if last:
            for p in range(1, pieces):
                if e > 0:
                    dpre_step(0, f, e, p)
                own_parts(p)
        else:
            for p in range(1, pieces):
                dpre_landed(partner, e, p)
        for p in range(pieces):
            dpre_step(1, across, e, p)
            if last:
                cross_part(2, p)
            dpre_landed(corner, e, p)
            if last:
                cross_part(3, p)
        if e == 0:
            for p in range(strips):
                @pl.when(jnp.logical_not(direct))
                def _():
                    cross_rest(1, p)

                line_landed(1, p)
        for q in range(tiles):
            up_step(e, q)
    for p in range(pieces):
        for k in range(2):
            own_sum(k, p)
    for p in range(pieces):
        for k in range(2, 4):
            cross_sum(k, p)

    relays = lax.div(z_far, 2) != place
    for p in range(pieces):
        @pl.when(relays)
        def _():
            ref = gi_mid.at[half_rows(p)]
            landed(ref, mid_recv.at[p])
            remote(
                ref, gi_in.at[1, half_rows(p)], relay_send.at[p], gi_recv.at[1, p], {"tp": z_far}
            ).start()

    for p in range(1, reps):
        for c in range(steps):
            rep_copy(gd_out, gd_in, gd_send, gd_recv, (c,), p).wait()
    for p in range(pieces):
        @pl.when(jnp.logical_not(home))
        def _():
            landed(gi_in.at[0, half_rows(p)], gi_recv.at[0, p])

        landed(gi_in.at[1, half_rows(p)], gi_recv.at[1, p])

        @pl.when(same)
        def _():
            landed(gi_in.at[2, half_rows(p)], gi_recv.at[2, p])

    for p in range(strips):
        for a in range(2):
            @pl.when(same & (z != f) | jnp.logical_not(same))
            def _():
                left_for(own.at[pl.ds(p * sp, sp)], org_send.at[a, 0, p])

            @pl.when(direct)
            def _():
                for source in (across, corner):
                    left_for(own.at[pl.ds(p * sp, sp)], fwd_send.at[a, source, p])

        @pl.when(jnp.logical_not(same))
        def _():
            for a in range(2):
                left_for(own.at[pl.ds(p * sp, sp)], org_send.at[a, 1, p])

        @pl.when(same & (z < T - 1))
        def _():
            left_for(own.at[pl.ds(p * sp, sp)], org_send.at[0, 1, p])

        @pl.when(same & (z > 0))
        def _():
            left_for(own.at[pl.ds(p * sp, sp)], org_send.at[0, 2, p])

        @pl.when(rises | falls)
        def _():
            for source in (f, partner):
                left_for(own.at[pl.ds(p * sp, sp)], fwd_send.at[0, source, p])

        for k in range(1, T - 1):
            @pl.when(same & ((z + k < T - 1) | ((k == 1) & (z + k < T))))
            def _():
                left_for(own.at[pl.ds(p * sp, sp)], org_send.at[1, T + k, p])

            @pl.when(same & ((z - k > 0) | ((k == 1) & (z - k >= 0))))
            def _():
                left_for(own.at[pl.ds(p * sp, sp)], org_send.at[1, 1 + k, p])

        @pl.when(last_up | last_down)
        def _():
            for source in (f, partner):
                left_for(own.at[pl.ds(p * sp, sp)], fwd_send.at[1, source, p])

    for p in range(pieces):
        @pl.when(jnp.logical_not(home))
        def _():
            left_for(own.at[half_rows(p)], gi_send.at[0, p])

        for k in range(1, 4):
            left_for(own.at[half_rows(p)], gi_send.at[k, p])

        @pl.when(relays)
        def _():
            left_for(own.at[half_rows(p)], relay_send.at[p])

        for k in range(2):
            left_for(pair_out.at[k, p], pair_send.at[k, p])
            for e in range(parts):
                left_for(dpre_group.at[piece(f, p), hidden(e)], dpre_send.at[k, e, p])
                left_for(far_out.at[k, e, p], far_send.at[k, e, p])
    for k in range(3):
        for c in range(steps):
            left_for(pos_group.at[rows(f), act_cols(c)], act_send.at[k, c])
    for p in range(1, reps):
        for e in range(parts):
            for q in range(tiles):
                rep_copy(gu_out, gu_in, gu_send, gu_recv, (e, q), p).wait()


def finish_kernel(
    gd_out, gd_in, gu_out, gu_in, gi_in, grad_input, grad_up, grad_down,
    gi_v, gu_v, gd_v, gi_sem, gu_sem, gd_sem,
):
    others = gd_in.shape[0]
    steps, gd_rows = gd_out.shape[0], gd_out.shape[1]
    parts, tiles, gu_rows, hp = gu_out.shape
    copies = []

    def leave(src, dst, sem):
        copies.append(pltpu.make_async_copy(src, dst, sem))
        copies[-1].start()

    for c in range(steps):
        value = gd_out[c].astype(F32)
        for p in range(others):
            value = value + gd_in[p, c].astype(F32)
        gd_v[c] = value
        leave(gd_v.at[c], grad_down.at[pl.ds(c * gd_rows, gd_rows)], gd_sem.at[c])
    for e in range(parts):
        for q in range(tiles):
            value = gu_out[e, q].astype(F32)
            for p in range(others):
                value = value + gu_in[p, e, q].astype(F32)
            gu_v[e, q] = value
            at = (pl.ds(q * gu_rows, gu_rows), pl.ds(e * hp, hp))
            leave(gu_v.at[e, q], grad_up.at[at], gu_sem.at[e, q])
    value = gi_in[0].astype(F32)
    for s in range(1, gi_in.shape[0]):
        value = value + gi_in[s].astype(F32)
    gi_v[...] = value.astype(BF16)
    leave(gi_v, grad_input, gi_sem.at[0])
    for copy in copies:
        copy.wait()


def square_body(sizes, acts, cotangent, pre_act, up_store, up_scale, down_store, down_scale):
    reps, F, T = sizes
    n, d = acts.shape
    h = pre_act.shape[1]
    w = down_store.shape[1]
    parts = 2 if h % 256 == 0 else 1
    pieces = 2 if n % 32 == 0 else 1
    tiles = 2 if w % 256 == 0 else 1
    strips = 2 * pieces if n % 64 == 0 else pieces
    hp, rp = h // parts, n // pieces
    gd_rows = fitting(h, 256)
    steps = h // gd_rows
    others = reps - 1
    sem = pltpu.SemaphoreType.DMA
    vmem, hbm = (pl.BlockSpec(memory_space=s) for s in (pltpu.VMEM, pltpu.HBM))
    shared = [
        (steps, gd_rows, w), (others, steps, gd_rows, w),
        (parts, tiles, w // tiles, hp), (others, parts, tiles, w // tiles, hp),
        (3, n, w),
    ]
    arrays = [
        ((n, d), BF16), ((n, d), BF16), ((n, h), BF16),
        ((w, h), F32), ((1, h), F32), ((h, w), F32), ((1, d * T), F32),
        ((n, d), BF16), ((F * n, w), BF16), ((F * n, w), BF16),
        ((F * n, h), BF16), ((F * n, h), BF16),
        ((w, h), BF16), ((h, w), BF16),
        ((2, pieces, rp, h), BF16), ((2, pieces, rp, h), BF16),
        ((2, parts, pieces, rp, hp), BF16), ((2, parts, pieces, rp, hp), BF16),
        ((2, pieces, rp, h), F32),
        ((F, n, w), BF16), ((n, w), BF16), ((F, n, w), BF16), ((F, n, w), F32),
    ]
    moved = pl.pallas_call(
        functools.partial(square_kernel, sizes),
        out_shape=tuple(jax.ShapeDtypeStruct(shape, BF16) for shape in shared),
        in_specs=[hbm] * 7,
        out_specs=(vmem,) * len(shared),
        scratch_shapes=[pltpu.VMEM(shape, kind) for shape, kind in arrays] + [
            sem((7,)),
            sem((2, 2 * T, strips)), sem((2, F, strips)), sem((2, F, strips)),
            sem((3, steps)), sem((F, steps)), sem((2, parts, pieces)), sem((parts, F, pieces)),
            sem((2, pieces)), sem((2, pieces)), sem((2, parts, pieces)), sem((2, parts, pieces)),
            sem((pieces,)), sem((F, pieces)), sem((F, pieces)), sem((3, pieces)), sem((pieces,)),
            sem((others, steps)), sem((others, steps)),
            sem((others, parts, tiles)), sem((others, parts, tiles)),
        ],
        compiler_params=pltpu.CompilerParams(
            collective_id=0, has_side_effects=True,
            vmem_limit_bytes=40 * 1024 * 1024,
        ),
    )(*(
        pltpu.with_memory_space_constraint(array, pltpu.HBM)
        for array in (
            acts, cotangent, pre_act, up_store, up_scale.reshape(1, h), down_store,
            down_scale.reshape(1, d * T),
        )
    ))
    return pl.pallas_call(
        finish_kernel,
        out_shape=(
            jax.ShapeDtypeStruct((n, d), BF16),
            jax.ShapeDtypeStruct((w, h), F32),
            jax.ShapeDtypeStruct((h, w), F32),
        ),
        in_specs=[vmem] * len(shared),
        out_specs=(hbm,) * 3,
        scratch_shapes=[
            pltpu.VMEM((n, d), BF16),
            pltpu.VMEM((parts, tiles, w // tiles, hp), F32),
            pltpu.VMEM((steps, gd_rows, w), F32),
            sem((1,)), sem((parts, tiles)), sem((steps,)),
        ],
        compiler_params=pltpu.CompilerParams(vmem_limit_bytes=12 * 1024 * 1024),
    )(*moved)


def body(sizes, *arrays):
    reps, F, T = sizes
    square = F == T and F == 2 * 2 and reps > 1
    return (square_body if square else general_body)(sizes, *arrays)


def solution(mesh):
    sizes = (mesh.shape["rep"], mesh.shape["fs"], mesh.shape["tp"])
    return jax.shard_map(
        functools.partial(body, sizes),
        mesh=mesh,
        in_specs=(
            P(("rep", "fs"), "tp"),
            P(("rep", "fs"), "tp"),
            P(("rep", "fs"), "tp"),
            P("fs", "tp"),
            P("tp"),
            P("tp", "fs"),
            P(),
        ),
        out_specs=(P(("rep", "fs"), "tp"), P("fs", "tp"), P("tp", "fs")),
        check_vma=False,
    )
```
